1024 devices in a mesh: kv: 256 (over z, y, core), tp: 4 (over x).
Axes of the slice: x: 4, y: 8, z: 16, core: 2. Of those that a mesh axis runs over, the one named last changes fastest.
Arguments:
- layer_input: bfloat16 [49152, 2048], P('kv', 'tp'), may hold values from -0.109375 to 0.109375
- queries: bfloat16 [49152, 1024], P('kv', 'tp'), may hold values from -6 to 6
- keys: bfloat16 [49152, 256], P('kv', 'tp'), may hold values from -6 to 6
- values: bfloat16 [49152, 256], P('kv', 'tp'), may hold values from -6 to 6
- attn_out: bfloat16 [49152, 1024], P('kv', 'tp'), may hold values from -1.25 to 1.25
- grad_out: bfloat16 [49152, 1024], P('kv', 'tp'), may hold values from -128 to 128
- log_sum: float32 [49152, 16], P('kv', 'tp'), may hold values from 6 to 7.5
- chosen: int32 [768, 8], replicated, may hold values from -1 to 767, as said below
Outputs:
- grad_queries: bfloat16 [49152, 1024], P('kv', 'tp')
- grad_keys: bfloat16 [49152, 256], P('kv', 'tp')
- grad_values: bfloat16 [49152, 256], P('kv', 'tp')
- grad_weight: float32 [2048, 1024], P('kv', 'tp')
The draws below stay inside these ranges and needn't reach their ends.
Inputs may be any that keep to these rules, and one draw needn't show every extreme that they name: Write R = 3 and call positions [s * 192, (s + 1) * 192) segment s. For query block b in segment c = b // R and level l < 4, the entries chosen[b, 2 l + i] for i < 2 name 2 different key blocks of segment c - g_l, with g = 1, 32, 64, 128; all of them are -1 where c - g_l is negative.
All inputs are finite; a program needn't handle non-finite values.
Results may differ from the reference program's by a relative error of at most 0.0053.
Values may be sent and summed in bfloat16 or wider, within the bound.
No kernel may reach another device: no remote copies, remote signals or barrier semaphores. Data moves between devices by JAX's collectives and lax.ppermute only.
A program may use at most 64 MiB of HBM per device.

```python
import jax
import jax.numpy as jnp
from jax import lax

D = 2048
HEADS = 16
KVH = 4
DH = 64
BLOCK = 64
PER = 2
LEVELS = 4
TOK_DEV = 192
TOKENS = 49152
TOPK = 8
HOP = 32


def draw_chosen(key, part):
    per_segment = TOK_DEV // BLOCK
    total_blocks = TOKENS // BLOCK
    distances = jnp.array([1, HOP, 2 * HOP, 4 * HOP], jnp.int32)
    block_ids = jnp.arange(total_blocks, dtype=jnp.int32)
    segment = block_ids // per_segment
    ranks = jax.random.randint(jax.random.fold_in(key, 17), (total_blocks, LEVELS, per_segment), 0, 1 << 20)
    ranks = ranks * per_segment + jnp.arange(per_segment, dtype=jnp.int32)
    unused, order = lax.top_k(ranks, PER)
    source = segment[:, None] - distances[None, :]
    picked = source[:, :, None] * per_segment + order.astype(jnp.int32)
    picked = jnp.where(source[:, :, None] >= 0, picked, -1)
    return picked.reshape(total_blocks, LEVELS * PER).astype(jnp.int32)


def spiked(values, own_key, source, target, parts, factor):
    def block_of(position):
        return (jnp.arange(values.shape[position]) // (values.shape[position] // parts)).reshape((-1,) + (1,) * (values.ndim - 1 - position))

    one_side = jax.random.permutation(own_key, parts)[block_of(target)]
    far = (block_of(target) + parts // 2) % parts
    return jnp.where((block_of(source) == one_side) | (block_of(source) == far), factor * values, values)


def level_of(own_key, extent, cuts, least, largest):
    gain, own = 1.0, jax.random.fold_in(own_key, 6)
    for axis_at, blocks in cuts:
        draws = jnp.exp(jax.random.uniform(jax.random.fold_in(own, axis_at), (blocks,), jnp.float32, least / len(cuts), largest / len(cuts)))
        gain = gain * jnp.repeat(draws, extent[axis_at] // blocks).reshape([-1 if axis == axis_at else 1 for axis in range(len(extent))])
    return gain


def centred(stream_key, dims, deviation, limit, cuts=(), held_as=jnp.bfloat16):
    result = deviation * jax.random.normal(stream_key, dims, jnp.float32)
    if cuts:
        result = result * level_of(stream_key, dims, cuts, -0.22, 0.18)
    return jnp.clip(result, -limit, limit).astype(held_as)


def heavy_noise(key, shape, spread, most, cuts, heavy, kind=jnp.bfloat16):
    entries = spread * jax.random.normal(key, shape, jnp.float32)
    if cuts:
        entries = entries * level_of(key, shape, cuts, -0.22, 0.18)
    return jnp.clip(spiked(entries, jax.random.fold_in(key, 3), *heavy), -most, most).astype(kind)


def setup_inputs(seed: int = 0) -> dict:
    streams_of = jax.random.split(jax.random.key(seed), 9)
    layer_input = heavy_noise(streams_of[0], (TOKENS, D), (TOKENS ** -0.5), 0.109375, ((0, 256), (1, 4)), (0, 1, 256, 6.0))
    queries = centred(streams_of[1], (TOKENS, HEADS * DH), 1.0, 6.0, ((0, 256), (1, 4)))
    keys = centred(streams_of[2], (TOKENS, KVH * DH), 1.0, 6.0, ((0, 256), (1, 4)))
    values = centred(streams_of[3], (TOKENS, KVH * DH), 1.0, 6.0, ((0, 256), (1, 4)))
    attn_out = centred(streams_of[4], (TOKENS, HEADS * DH), 0.2, 1.25, ((0, 256), (1, 4)))
    grad_out = centred(streams_of[5], (TOKENS, HEADS * DH), 24.0, 128.0, ((0, 256), (1, 4)))
    log_sum = jnp.clip(6.0 + 1.5 * jax.random.uniform(streams_of[6], (TOKENS, HEADS), jnp.float32) ** level_of(streams_of[6], (TOKENS, HEADS), ((0, 256), (1, 4)), -0.2, 0.2), 6.0, 7.5)
    chosen = draw_chosen(jax.random.fold_in(streams_of[8], 71), 0)
    return {"layer_input": layer_input, "queries": queries, "keys": keys, "values": values, "attn_out": attn_out, "grad_out": grad_out, "log_sum": log_sum, "chosen": chosen}


def pair_terms(query_blk, grad_blk, lse_blk, delta_blk, key_blk, value_blk, keep_mask, scale_value):
    query_f = query_blk.astype(jnp.float32)
    grad_f = grad_blk.astype(jnp.float32)
    key_f = key_blk.astype(jnp.float32)
    value_f = value_blk.astype(jnp.float32)
    scores = jnp.einsum('pbkge,pcke->pkgbc', query_f, key_f) * scale_value
    lse_cols = jnp.transpose(lse_blk, (0, 2, 3, 1))[..., None]
    delta_cols = jnp.transpose(delta_blk, (0, 2, 3, 1))[..., None]
    weights = jnp.where(keep_mask[:, None, None], jnp.exp(scores - lse_cols), jnp.float32(0.0))
    weights_low = lax.optimization_barrier(weights.astype(jnp.bfloat16)).astype(jnp.float32)
    dweights = jnp.einsum('pbkge,pcke->pkgbc', grad_f, value_f)
    dscores = lax.optimization_barrier((weights * (dweights - delta_cols)).astype(jnp.bfloat16)).astype(jnp.float32)
    grad_query = jnp.einsum('pkgbc,pcke->pbkge', dscores, key_f) * scale_value
    grad_key = jnp.einsum('pkgbc,pbkge->pcke', dscores, query_f) * scale_value
    grad_value = jnp.einsum('pkgbc,pbkge->pcke', weights_low, grad_f)
    return grad_query, grad_key, grad_value


def reference(layer_input, queries, keys, values, attn_out, grad_out, log_sum, chosen):
    total_rows = queries.shape[0]
    nblocks = total_rows // BLOCK
    group_size = HEADS // KVH
    scale_value = DH ** -0.5
    query_all = queries.reshape(nblocks, BLOCK, KVH, group_size, DH)
    grad_all = grad_out.reshape(nblocks, BLOCK, KVH, group_size, DH)
    delta_all = jnp.sum(grad_out.astype(jnp.float32).reshape(nblocks, BLOCK, KVH, group_size, DH)
                        * attn_out.astype(jnp.float32).reshape(nblocks, BLOCK, KVH, group_size, DH), axis=-1)
    lse_all = log_sum.reshape(nblocks, BLOCK, KVH, group_size)
    key_all = keys.reshape(nblocks, BLOCK, KVH, DH)
    value_all = values.reshape(nblocks, BLOCK, KVH, DH)
    causal = lax.broadcasted_iota(jnp.int32, (BLOCK, BLOCK), 0) >= lax.broadcasted_iota(jnp.int32, (BLOCK, BLOCK), 1)
    slot_ids = jnp.arange(TOPK + 1, dtype=jnp.int32)

    def one_block(carry, block_num):
        key_acc, value_acc = carry
        listed = chosen[block_num].astype(jnp.int32)
        targets = jnp.concatenate([block_num[None], listed]).astype(jnp.int32)
        is_live = targets >= 0
        safe_ids = jnp.where(is_live, targets, 0).astype(jnp.int32)
        keep_mask = jnp.where((slot_ids == 0)[:, None, None], causal[None], True) & is_live[:, None, None]
        count_pairs = TOPK + 1
        query_rep = jnp.broadcast_to(query_all[block_num][None], (count_pairs, BLOCK, KVH, group_size, DH))
        grad_rep = jnp.broadcast_to(grad_all[block_num][None], (count_pairs, BLOCK, KVH, group_size, DH))
        lse_rep = jnp.broadcast_to(lse_all[block_num][None], (count_pairs, BLOCK, KVH, group_size))
        delta_rep = jnp.broadcast_to(delta_all[block_num][None], (count_pairs, BLOCK, KVH, group_size))
        grad_query, grad_key, grad_value = pair_terms(query_rep, grad_rep, lse_rep, delta_rep,
                                                      key_all[safe_ids], value_all[safe_ids], keep_mask, scale_value)
        key_acc = key_acc.at[safe_ids].add(grad_key)
        value_acc = value_acc.at[safe_ids].add(grad_value)
        return (key_acc, value_acc), jnp.sum(grad_query, axis=0)

    zeros_acc = jnp.zeros((nblocks, BLOCK, KVH, DH), jnp.float32)
    (key_acc, value_acc), grad_blocks = lax.scan(one_block, (zeros_acc, zeros_acc),
                                                 jnp.arange(nblocks, dtype=jnp.int32))
    grad_queries = grad_blocks.reshape(total_rows, HEADS * DH).astype(jnp.bfloat16)
    grad_keys = key_acc.reshape(total_rows, KVH * DH).astype(jnp.bfloat16)
    grad_values = value_acc.reshape(total_rows, KVH * DH).astype(jnp.bfloat16)
    grad_weight = jnp.dot(layer_input.T, grad_queries, preferred_element_type=jnp.float32)
    return grad_queries, grad_keys, grad_values, grad_weight
```

```python
import functools

import jax
import jax.numpy as jnp
from jax import lax
from jax.experimental import pallas as pl
from jax.experimental.pallas import tpu as pltpu
from jax.sharding import Mesh
from jax.sharding import PartitionSpec as P

DH = 64
BLOCK = 64
PER = 2
LEVELS = 4
SIDES = (8, 2)
KV = ("z", "y", "c")
NT = (((1,), (1,)), ((), ()))
TN = (((0,), (0,)), ((), ()))


def shifted(block, axis, distance):
    devices = range(lax.axis_size(axis))
    route = [(i - distance, i) for i in devices if i - distance in devices]
    return lax.ppermute(block, axis, route)


def exchanged(tiles, axis):
    return lax.all_to_all(tiles, axis, split_axis=0, concat_axis=0, tiled=True)


def dot(a, b, dims=(((1,), (0,)), ((), ()))):
    return lax.dot_general(a, b, dims, preferred_element_type=jnp.float32)


def spread_kernel(rows, ys, cores, peers, x_ref, out_ref):
    width = x_ref.shape[1]
    source = lax.broadcasted_iota(jnp.int32, (width, width), 0)
    target = lax.broadcasted_iota(jnp.int32, (width, width), 1)
    inner, left = source % rows, source // rows
    core, left = left % cores, left // cores
    y, z = left % ys, left // ys
    zs = width // (rows * cores * ys)
    place = ((core * ys + y) * zs + z) * rows + inner
    move = jnp.where(place == target, 1.0, 0.0).astype(jnp.bfloat16)
    moved = dot(x_ref[...], move).astype(jnp.bfloat16)
    part = width // cores
    for core in range(cores):
        for peer in range(peers):
            out_ref[core * peers + peer] = moved[:, core * part : (core + 1) * part]


def spread(x, rows, ys, cores, peers):
    tokens, width = x.shape
    return pl.pallas_call(
        functools.partial(spread_kernel, rows, ys, cores, peers),
        out_shape=jax.ShapeDtypeStruct((cores * peers, tokens, width // cores), x.dtype),
        cost_estimate=pl.CostEstimate(
            flops=2 * tokens * width * width, bytes_accessed=2 * tokens * width * (1 + peers), transcendentals=0
        ),
        name="spread",
    )(x)


def stacked(block, at):
    block = block.astype(jnp.float32)
    lane = lax.broadcasted_iota(jnp.int32, (BLOCK, 2 * DH), 1)
    keep = (lane >= at) & (lane < at + DH)
    parts = []
    for head in range(block.shape[1] // DH):
        pair = block[:, (head // 2) * 2 * DH : (head // 2 + 1) * 2 * DH]
        if (head % 2) * DH != at:
            pair = pltpu.roll(pair, DH, 1)
        parts.append(jnp.where(keep, pair, 0.0))
    return jnp.concatenate(parts, axis=0)


def row_sums(terms, pieces):
    ones = jnp.ones((8, terms.shape[1]), jnp.bfloat16)
    total = None
    for _ in range(pieces):
        piece = terms.astype(jnp.bfloat16)
        terms = terms - piece.astype(jnp.float32)
        part = dot(ones, piece, NT)
        total = part if total is None else total + part
    return total[:1]


def attention_kernel(
    offs_ref, q_ref, go_ref, ao_ref, lse_ref, k_ref, v_ref, *refs
):
    far_refs = refs[:LEVELS]
    gq_ref, own_ref = refs[LEVELS : LEVELS + 2]
    back_refs = refs[LEVELS + 2 : 2 * LEVELS + 2]
    sums = refs[2 * LEVELS + 2]
    blocks = q_ref.shape[0] // BLOCK
    heads = q_ref.shape[1] // DH
    own_kv = jnp.concatenate([k_ref[...], v_ref[...]], axis=1)
    lane = lax.broadcasted_iota(jnp.int32, (BLOCK, 2 * DH), 1)
    sums[...] = jnp.zeros_like(sums)
    key_at = lax.broadcasted_iota(jnp.int32, (BLOCK, heads * BLOCK), 0)
    query_at = lax.broadcasted_iota(jnp.int32, (BLOCK, heads * BLOCK), 1) % BLOCK
    causal = key_at <= query_at
    for b in range(blocks):
        rows = slice(b * BLOCK, (b + 1) * BLOCK)
        low = stacked(q_ref[rows] * DH ** (-0.5), 0)
        high = stacked(go_ref[rows], DH)
        delta = row_sums(high * stacked(ao_ref[rows], DH), 2)
        lse_rows = lse_ref[rows]
        lse = row_sums(
            jnp.concatenate(
                [jnp.where(lane == 0, lse_rows[:, h : h + 1], 0.0) for h in range(heads)], axis=0
            ),
            3,
        )
        low = low.astype(jnp.bfloat16)
        high = high.astype(jnp.bfloat16)
        places = [
            pl.multiple_of(offs_ref[b, n] * BLOCK, BLOCK) for n in range(LEVELS * PER)
        ]
        kv = jnp.concatenate(
            [own_kv[rows]]
            + [far_refs[n // PER][pl.ds(places[n], BLOCK), :] for n in range(LEVELS * PER)],
            axis=0,
        )
        weights = jnp.exp(dot(kv, low, NT) - lse)
        weights = jnp.concatenate(
            [jnp.where(causal, weights[:BLOCK], 0.0), weights[BLOCK:]], axis=0
        )
        dscores = (weights * (dot(kv, high, NT) - delta)).astype(jnp.bfloat16)
        grad_kv = dot(dscores, low) + dot(weights.astype(jnp.bfloat16), high)
        own_ref[rows] = grad_kv[:BLOCK]
        for n in range(LEVELS * PER):
            at = pl.ds(places[n], BLOCK)
            sums[n // PER, at, :] += grad_kv[(n + 1) * BLOCK : (n + 2) * BLOCK]
        grad_q = dot(dscores, kv, TN) * DH ** (-0.5)
        for pair in range(heads // 2):
            first = grad_q[2 * pair * BLOCK : (2 * pair + 1) * BLOCK]
            second = grad_q[(2 * pair + 1) * BLOCK : (2 * pair + 2) * BLOCK]
            gq_ref[rows, pair * 2 * DH : (pair + 1) * 2 * DH] = jnp.where(
                lane < DH, first, pltpu.roll(second, DH, 1)
            ).astype(gq_ref.dtype)
    for level in range(LEVELS):
        back_refs[level][...] = sums[level].astype(jnp.bfloat16)


def attention(offs, q, go, ao, lse, k, v, far):
    tokens, width = q.shape
    vmem = pl.BlockSpec(memory_space=pltpu.VMEM)
    return pl.pallas_call(
        attention_kernel,
        out_shape=(
            jax.ShapeDtypeStruct((tokens, width), jnp.bfloat16),
            jax.ShapeDtypeStruct((tokens, 2 * DH), jnp.float32),
        )
        + (jax.ShapeDtypeStruct((tokens, 2 * DH), jnp.bfloat16),) * LEVELS,
        in_specs=[pl.BlockSpec(memory_space=pltpu.SMEM)] + [vmem] * (6 + LEVELS),
        out_specs=(vmem,) * (2 + LEVELS),
        scratch_shapes=[pltpu.VMEM((LEVELS, tokens, 2 * DH), jnp.float32)],
        cost_estimate=pl.CostEstimate(flops=2 * 10**9, bytes_accessed=10**6, transcendentals=10**6),
        name="attention",
    )(offs, q, go, ao, lse, k, v, *far)


def weight_kernel(core_ref, mine_ref, other_ref, x_ref, out_ref):
    core = core_ref[0]
    peers = x_ref.shape[0] // 2
    ys = out_ref.shape[0]
    grads = jnp.concatenate([mine_ref[...], other_ref[...]], axis=0)
    for peer in range(peers):
        x = jnp.concatenate(
            [x_ref[core * peers + peer], x_ref[(1 - core) * peers + peer]], axis=0
        )
        part = dot(x, grads, TN).astype(out_ref.dtype)
        step = part.shape[0] // ys
        for y in range(ys):
            out_ref[y, peer * step : (peer + 1) * step] = part[y * step : (y + 1) * step]


def weight(core, mine, other, x, ys):
    peers, tokens, part = x.shape[0] // 2, x.shape[1], x.shape[2]
    vmem = pl.BlockSpec(memory_space=pltpu.VMEM)
    return pl.pallas_call(
        weight_kernel,
        out_shape=jax.ShapeDtypeStruct((ys, peers * part // ys, mine.shape[1]), jnp.bfloat16),
        in_specs=[pl.BlockSpec(memory_space=pltpu.SMEM), vmem, vmem, vmem],
        out_specs=vmem,
        cost_estimate=pl.CostEstimate(
            flops=4 * tokens * peers * part * mine.shape[1], bytes_accessed=2 * 10**6, transcendentals=0
        ),
        name="weight",
    )(core, mine, other, x)


def summed(tiles):
    return jnp.sum(tiles.astype(jnp.float32), axis=0)


def shards(layer_input, queries, keys, values, attn_out, grad_out, log_sum, chosen):
    axis_size = lax.axis_size(KV)
    my_index = lax.axis_index(KV)
    ys, cores, peers = lax.axis_size("y"), lax.axis_size("c"), lax.axis_size("x")
    tok_rows = queries.shape[0]
    blocks_here = tok_rows // BLOCK
    key_width = keys.shape[1]
    out_rows = layer_input.shape[1] * peers // axis_size
    distances = [1, axis_size // 8, axis_size // 4, axis_size // 2]
    key_pair = jnp.concatenate([keys, values], axis=1)
    far = [shifted(key_pair, KV, distance) for distance in distances]
    whole_input = exchanged(spread(layer_input, out_rows, ys, cores, peers), ("c", "x"))
    listed = lax.dynamic_slice(chosen, (my_index * blocks_here, 0), (blocks_here, LEVELS * PER))
    first = (my_index - jnp.repeat(jnp.array(distances, jnp.int32), PER)) * blocks_here
    offs = jnp.where(listed >= 0, listed - first, 0)
    grad_queries, own, *back = attention(
        offs, queries, grad_out, attn_out, log_sum, keys, values, far
    )
    other = lax.ppermute(grad_queries, "c", [(i, cores - 1 - i) for i in range(cores)])
    core = lax.axis_index("c").astype(jnp.int32).reshape(1)
    parts = weight(core, grad_queries, other, whole_input, ys)
    over_y = summed(exchanged(parts, "y")).astype(jnp.bfloat16)
    over_z = exchanged(over_y.reshape(-1, out_rows, over_y.shape[1]), "z")
    grad_weight = summed(over_z)
    for level, distance in enumerate(distances):
        own = own + shifted(back[level], KV, -distance).astype(jnp.float32)
    own = own.astype(jnp.bfloat16)
    return (grad_queries, own[:, :key_width], own[:, key_width:], grad_weight)


def solution(mesh):
    ys, cores = SIDES
    shape = (mesh.shape["kv"] // (ys * cores), ys, cores, mesh.shape["tp"])
    torus = Mesh(mesh.devices.reshape(shape), (*KV, "x"))
    return jax.shard_map(
        shards,
        mesh=torus,
        in_specs=(P(KV, "x"),) * 7 + (P(),),
        out_specs=(P(KV, "x"),) * 4,
        check_vma=False,
    )
```

```python
import functools

import jax
import jax.numpy as jnp
from jax import lax
from jax.experimental import pallas as pl
from jax.experimental.pallas import tpu as pltpu
from jax.sharding import Mesh
from jax.sharding import PartitionSpec as P

DH = 64
BLOCK = 64
PER = 2
LEVELS = 4
SIDES = (8, 2)
KV = ("z", "y", "c")
NT = (((1,), (1,)), ((), ()))
TN = (((0,), (0,)), ((), ()))
VMEM_LIMIT = 16 * 2**20


def shifted(block, axis, distance):
    devices = range(lax.axis_size(axis))
    route = [(i - distance, i) for i in devices if i - distance in devices]
    return lax.ppermute(block, axis, route)


def exchanged(tiles, axis):
    return lax.all_to_all(tiles, axis, split_axis=0, concat_axis=0, tiled=True)


def dot(a, b, dims=(((1,), (0,)), ((), ()))):
    return lax.dot_general(a, b, dims, preferred_element_type=jnp.float32)


def call(kernel, flops, out_shape, *args, smem=0, scratch=()):
    vmem = pl.BlockSpec(memory_space=pltpu.VMEM)
    many = isinstance(out_shape, tuple)
    size = sum(a.size * a.dtype.itemsize for a in args)
    return pl.pallas_call(
        kernel,
        out_shape=out_shape,
        in_specs=[pl.BlockSpec(memory_space=pltpu.SMEM)] * smem + [vmem] * (len(args) - smem),
        out_specs=(vmem,) * len(out_shape) if many else vmem,
        scratch_shapes=scratch,
        cost_estimate=pl.CostEstimate(flops=flops, bytes_accessed=size, transcendentals=0),
        compiler_params=pltpu.CompilerParams(vmem_limit_bytes=VMEM_LIMIT),
    )(*args)


def turned(x):
    return jnp.transpose(x.astype(jnp.float32))


def pack_kernel(k_ref, v_ref, out_ref):
    out_ref[...] = turned(jnp.concatenate([k_ref[...], v_ref[...]], axis=0)).astype(out_ref.dtype)


def pack(k, v):
    shape = jax.ShapeDtypeStruct((k.shape[1], 2 * k.shape[0]), k.dtype)
    return call(pack_kernel, 10**6, shape, k, v)


def spread_kernel(rows, ys, cores, peers, x_ref, out_ref):
    width = x_ref.shape[1]
    source = lax.broadcasted_iota(jnp.int32, (width, 1), 0)
    target = lax.broadcasted_iota(jnp.int32, (width, width), 1)
    inner, left = source & (rows - 1), source // rows
    core, left = left & (cores - 1), left // cores
    y, z = left & (ys - 1), left // ys
    zs = width // (rows * cores * ys)
    place = ((core * ys + y) * zs + z) * rows + inner
    move = jnp.where(place == target, 1.0, 0.0).astype(jnp.bfloat16)
    moved = dot(x_ref[...], move).astype(jnp.bfloat16)
    part = width // cores
    for core in range(cores):
        for peer in range(peers):
            out_ref[core * peers + peer] = moved[:, core * part : (core + 1) * part]


def spread(x, rows, ys, cores, peers):
    tokens, width = x.shape
    kernel = functools.partial(spread_kernel, rows, ys, cores, peers)
    shape = jax.ShapeDtypeStruct((cores * peers, tokens, width // cores), x.dtype)
    return call(kernel, 2 * tokens * width * width, shape, x)


def stacked(block, at):
    block = block.astype(jnp.float32)
    lane = lax.broadcasted_iota(jnp.int32, (BLOCK, 2 * DH), 1)
    keep = (lane >= at) & (lane < at + DH)
    parts = []
    for head in range(block.shape[1] // DH):
        pair = block[:, (head // 2) * 2 * DH : (head // 2 + 1) * 2 * DH]
        if (head % 2) * DH != at:
            pair = pltpu.roll(pair, DH, 1)
        parts.append(jnp.where(keep, pair, 0.0))
    return jnp.concatenate(parts, axis=0)


def row_sums(terms, pieces):
    ones = jnp.ones((8, terms.shape[1]), jnp.bfloat16)
    total = None
    for _ in range(pieces):
        piece = terms.astype(jnp.bfloat16)
        terms = terms - piece.astype(jnp.float32)
        part = dot(ones, piece, NT)
        total = part if total is None else total + part
    return total[:1]


def attention_kernel(distances, chosen_ref, q_ref, go_ref, ao_ref, lse_ref, kv_ref, *refs):
    far_refs = refs[:LEVELS]
    gq_ref, own_ref = refs[LEVELS : LEVELS + 2]
    back_refs = refs[LEVELS + 2 : 2 * LEVELS + 2]
    sums = refs[2 * LEVELS + 2]
    blocks = q_ref.shape[0] // BLOCK
    heads = q_ref.shape[1] // DH
    me = lax.axis_index(KV)
    lane = lax.broadcasted_iota(jnp.int32, (BLOCK, 2 * DH), 1)
    sums[...] = jnp.zeros_like(sums)
    key_at = lax.broadcasted_iota(jnp.int32, (BLOCK, heads * BLOCK), 0)
    query_at = lax.broadcasted_iota(jnp.int32, (BLOCK, heads * BLOCK), 1) & (BLOCK - 1)
    causal = key_at <= query_at
    for b in range(blocks):
        rows = slice(b * BLOCK, (b + 1) * BLOCK)
        low = stacked(q_ref[rows] * DH ** (-0.5), 0)
        high = stacked(go_ref[rows], DH)
        delta = row_sums(high * stacked(ao_ref[rows], DH), 2)
        lse = jnp.concatenate([lse_ref[h : h + 1, rows] for h in range(heads)], axis=1)
        low = low.astype(jnp.bfloat16)
        high = high.astype(jnp.bfloat16)
        places = []
        for n in range(LEVELS * PER):
            block = chosen_ref[n, me * blocks + b]
            block = jnp.where(block >= 0, block - (me - distances[n // PER]) * blocks, 0)
            places.append(pl.multiple_of(block * BLOCK, BLOCK))
        kv = jnp.concatenate(
            [kv_ref[rows]]
            + [far_refs[n // PER][pl.ds(places[n], BLOCK), :] for n in range(LEVELS * PER)],
            axis=0,
        )
        weights = jnp.exp(dot(kv, low, NT) - lse)
        weights = jnp.concatenate(
            [jnp.where(causal, weights[:BLOCK], 0.0), weights[BLOCK:]], axis=0
        )
        dscores = (weights * (dot(kv, high, NT) - delta)).astype(jnp.bfloat16)
        grad_kv = dot(dscores, low) + dot(weights.astype(jnp.bfloat16), high)
        own_ref[rows] = grad_kv[:BLOCK]
        for n in range(LEVELS * PER):
            at = pl.ds(places[n], BLOCK)
            sums[n // PER, at, :] += grad_kv[(n + 1) * BLOCK : (n + 2) * BLOCK]
        grad_q = dot(dscores, kv, TN) * DH ** (-0.5)
        for pair in range(heads // 2):
            first = grad_q[2 * pair * BLOCK : (2 * pair + 1) * BLOCK]
            second = grad_q[(2 * pair + 1) * BLOCK : (2 * pair + 2) * BLOCK]
            gq_ref[rows, pair * 2 * DH : (pair + 1) * 2 * DH] = jnp.where(
                lane < DH, first, pltpu.roll(second, DH, 1)
            ).astype(gq_ref.dtype)
    for level in range(LEVELS):
        back_refs[level][...] = sums[level].astype(jnp.bfloat16)


def attention(distances, chosen, q, go, ao, lse, kv, far):
    tokens, width = q.shape
    shape = (jax.ShapeDtypeStruct((tokens, width), jnp.bfloat16),)
    shape += (jax.ShapeDtypeStruct(kv.shape, jnp.float32),)
    shape += (jax.ShapeDtypeStruct(kv.shape, jnp.bfloat16),) * LEVELS
    return call(
        functools.partial(attention_kernel, distances),
        2 * 10**9,
        shape,
        chosen,
        q,
        go,
        ao,
        lse,
        kv,
        *far,
        smem=1,
        scratch=[pltpu.VMEM((LEVELS, *kv.shape), jnp.float32)],
    )


def weight_kernel(mine_ref, other_ref, x_ref, out_ref):
    core = lax.axis_index("c")
    peers = x_ref.shape[0] // 2
    ys = out_ref.shape[0]
    grads = jnp.concatenate([mine_ref[...], other_ref[...]], axis=0)
    for peer in range(peers):
        x = jnp.concatenate(
            [x_ref[core * peers + peer], x_ref[(1 - core) * peers + peer]], axis=0
        )
        part = dot(x, grads, TN).astype(out_ref.dtype)
        step = part.shape[0] // ys
        for y in range(ys):
            out_ref[y, peer * step : (peer + 1) * step] = part[y * step : (y + 1) * step]


def weight(mine, other, x, ys):
    peers, tokens, part = x.shape[0] // 2, x.shape[1], x.shape[2]
    shape = jax.ShapeDtypeStruct((ys, peers * part // ys, mine.shape[1]), jnp.bfloat16)
    flops = 4 * tokens * peers * part * mine.shape[1]
    return call(weight_kernel, flops, shape, mine, other, x)


def sum_kernel(tiles_ref, out_ref):
    total = tiles_ref[0].astype(jnp.float32)
    for n in range(1, tiles_ref.shape[0]):
        total = total + tiles_ref[n].astype(jnp.float32)
    out_ref[...] = total.astype(out_ref.dtype)


def summed(tiles, dtype):
    shape = jax.ShapeDtypeStruct(tiles.shape[1:], dtype)
    return call(sum_kernel, tiles.size, shape, tiles)


def collect_kernel(own_ref, *refs):
    total = own_ref[...]
    for ref in refs[:LEVELS]:
        total = total + ref[...].astype(jnp.float32)
    total = turned(total)
    width = total.shape[0] // 2
    refs[LEVELS][...] = total[:width].astype(jnp.bfloat16)
    refs[LEVELS + 1][...] = total[width:].astype(jnp.bfloat16)


def collect(own, back):
    shape = jax.ShapeDtypeStruct((own.shape[1] // 2, own.shape[0]), jnp.bfloat16)
    return call(collect_kernel, 10**6, (shape, shape), own, *back)


def shards(layer_input, queries, keys, values, attn_out, grad_out, log_sum, chosen):
    axis_size = lax.axis_size(KV)
    ys, cores, peers = lax.axis_size("y"), lax.axis_size("c"), lax.axis_size("x")
    out_rows = layer_input.shape[1] * peers // axis_size
    distances = [1, axis_size // 8, axis_size // 4, axis_size // 2]
    key_pair = pack(keys.T, values.T)
    far = []
    for distance in distances:
        far.append(shifted(key_pair, KV, distance))
    sent = spread(layer_input, out_rows, ys, cores, peers)
    whole_input = exchanged(sent, ("c", "x"))
    grad_queries, own, *back = attention(
        distances, chosen.T, queries, grad_out, attn_out, log_sum.T, key_pair, far
    )
    route = [(i, cores - 1 - i) for i in range(cores)]
    other = lax.ppermute(grad_queries, "c", route)
    parts = weight(grad_queries, other, whole_input, ys)
    over_y = exchanged(parts, "y")
    returned = []
    for level, distance in enumerate(distances):
        returned.append(shifted(back[level], KV, -distance))
    over_y = summed(over_y.reshape(ys, -1, out_rows, over_y.shape[2]), jnp.bfloat16)
    over_z = exchanged(over_y, "z")
    grad_keys, grad_values = collect(own, returned)
    grad_weight = summed(over_z, jnp.float32)
    return (grad_queries, grad_keys.T, grad_values.T, grad_weight)


def solution(mesh):
    ys, cores = SIDES
    shape = (mesh.shape["kv"] // (ys * cores), ys, cores, mesh.shape["tp"])
    torus = Mesh(mesh.devices.reshape(shape), (*KV, "x"))
    return jax.shard_map(
        shards,
        mesh=torus,
        in_specs=(P(KV, "x"),) * 7 + (P(),),
        out_specs=(P(KV, "x"),) * 4,
        check_vma=False,
    )
```

```python
import functools

import jax
import jax.numpy as jnp
from jax import lax
from jax.experimental import pallas as pl
from jax.experimental.pallas import tpu as pltpu
from jax.sharding import Mesh
from jax.sharding import PartitionSpec as P

DH = 64
BLOCK = 64
PER = 2
LEVELS = 4
SIDES = (8, 2)
KV = ("z", "y", "c")
NT = (((1,), (1,)), ((), ()))
TN = (((0,), (0,)), ((), ()))
VMEM_LIMIT = 16 * 2**20


def shifted(block, axis, distance):
    devices = range(lax.axis_size(axis))
    route = [(i - distance, i) for i in devices if i - distance in devices]
    return lax.ppermute(block, axis, route)


def between(block, quarters, pairs):
    route = [p for a, b in pairs for p in zip(quarters[a], quarters[b])]
    return lax.ppermute(block, "z", route)


def exchanged(tiles, axis):
    return lax.all_to_all(tiles, axis, split_axis=0, concat_axis=0, tiled=True)


def dot(a, b, dims=(((1,), (0,)), ((), ()))):
    return lax.dot_general(a, b, dims, preferred_element_type=jnp.float32)


def call(kernel, flops, out_shape, *args, smem=0, scratch=()):
    vmem = pl.BlockSpec(memory_space=pltpu.VMEM)
    many = isinstance(out_shape, tuple)
    size = sum(a.size * a.dtype.itemsize for a in args)
    return pl.pallas_call(
        kernel,
        out_shape=out_shape,
        in_specs=[pl.BlockSpec(memory_space=pltpu.SMEM)] * smem + [vmem] * (len(args) - smem),
        out_specs=(vmem,) * len(out_shape) if many else vmem,
        scratch_shapes=scratch,
        cost_estimate=pl.CostEstimate(flops=flops, bytes_accessed=size, transcendentals=0),
        compiler_params=pltpu.CompilerParams(vmem_limit_bytes=VMEM_LIMIT),
    )(*args)


def turned(x):
    return jnp.transpose(x.astype(jnp.float32))


def pack_kernel(kv_ref, out_ref):
    out_ref[...] = turned(kv_ref[...]).astype(out_ref.dtype)


def pack(k, v):
    kv = jnp.concatenate([k, v], axis=0)
    shape = jax.ShapeDtypeStruct(kv.shape[::-1], kv.dtype)
    return call(pack_kernel, 10**10, shape, kv)


def spread_kernel(rows, ys, cores, peers, x_ref, out_ref):
    width = x_ref.shape[1]
    source = lax.broadcasted_iota(jnp.int32, (width, 1), 0)
    target = lax.broadcasted_iota(jnp.int32, (width, width), 1)
    inner, left = source & (rows - 1), source // rows
    core, left = left & (cores - 1), left // cores
    y, z = left & (ys - 1), left // ys
    zs = width // (rows * cores * ys)
    place = ((core * ys + y) * zs + z) * rows + inner
    move = jnp.where(place == target, 1.0, 0.0).astype(jnp.bfloat16)
    moved = dot(x_ref[...], move).astype(jnp.bfloat16)
    part = width // cores
    for core in range(cores):
        for peer in range(peers):
            out_ref[core * peers + peer] = moved[:, core * part : (core + 1) * part]


def spread(x, rows, ys, cores, peers):
    tokens, width = x.shape
    kernel = functools.partial(spread_kernel, rows, ys, cores, peers)
    shape = jax.ShapeDtypeStruct((cores * peers, tokens, width // cores), x.dtype)
    return call(kernel, 2 * tokens * width * width, shape, x)


def stacked(block, at):
    block = block.astype(jnp.float32)
    lane = lax.broadcasted_iota(jnp.int32, (BLOCK, 2 * DH), 1)
    keep = (lane >= at) & (lane < at + DH)
    parts = []
    for head in range(block.shape[1] // DH):
        pair = block[:, (head // 2) * 2 * DH : (head // 2 + 1) * 2 * DH]
        if (head % 2) * DH != at:
            pair = pltpu.roll(pair, DH, 1)
        parts.append(jnp.where(keep, pair, 0.0))
    return jnp.concatenate(parts, axis=0)


def row_sums(terms, pieces):
    ones = jnp.ones((8, terms.shape[1]), jnp.bfloat16)
    total = None
    for _ in range(pieces):
        piece = terms.astype(jnp.bfloat16)
        terms = terms - piece.astype(jnp.float32)
        part = dot(ones, piece, NT)
        total = part if total is None else total + part
    return total[:1]


def attention_kernel(distances, chosen_ref, q_ref, go_ref, ao_ref, lse_ref, kv_ref, *refs):
    one_ref, two_ref, traded_ref, fetched_ref, passed_ref = refs[: LEVELS + 1]
    gq_ref, gq_too_ref, own_ref = refs[LEVELS + 1 : LEVELS + 4]
    back_refs = refs[LEVELS + 4 : 2 * LEVELS + 4]
    sums, four_ref = refs[2 * LEVELS + 4 :]
    at, quarter = lax.axis_index("z"), lax.axis_size("z") // 4
    in_second = jnp.logical_and(at >= quarter, at < 2 * quarter)
    four_ref[...] = jnp.where(in_second, traded_ref[...], fetched_ref[...])
    far_refs = (one_ref, two_ref, four_ref, passed_ref)
    blocks = q_ref.shape[0] // BLOCK
    heads = q_ref.shape[1] // DH
    me = lax.axis_index(KV)
    lane = lax.broadcasted_iota(jnp.int32, (BLOCK, 2 * DH), 1)
    sums[...] = jnp.zeros_like(sums)
    key_at = lax.broadcasted_iota(jnp.int32, (BLOCK, heads * BLOCK), 0)
    query_at = lax.broadcasted_iota(jnp.int32, (BLOCK, heads * BLOCK), 1) & (BLOCK - 1)
    causal = key_at <= query_at
    for b in range(blocks):
        rows = slice(b * BLOCK, (b + 1) * BLOCK)
        low = stacked(q_ref[rows] * DH ** (-0.5), 0)
        high = stacked(go_ref[rows], DH)
        delta = row_sums(high * stacked(ao_ref[rows], DH), 2)
        lse = jnp.concatenate([lse_ref[h : h + 1, rows] for h in range(heads)], axis=1)
        low = low.astype(jnp.bfloat16)
        high = high.astype(jnp.bfloat16)
        places = []
        for n in range(LEVELS * PER):
            block = chosen_ref[n, me * blocks + b]
            block = jnp.where(block >= 0, block - (me - distances[n // PER]) * blocks, 0)
            places.append(pl.multiple_of(block * BLOCK, BLOCK))
        kv = jnp.concatenate(
            [kv_ref[rows]]
            + [far_refs[n // PER][pl.ds(places[n], BLOCK), :] for n in range(LEVELS * PER)],
            axis=0,
        )
        weights = jnp.exp(dot(kv, low, NT) - lse)
        weights = jnp.concatenate(
            [jnp.where(causal, weights[:BLOCK], 0.0), weights[BLOCK:]], axis=0
        )
        dscores = (weights * (dot(kv, high, NT) - delta)).astype(jnp.bfloat16)
        grad_kv = dot(dscores, low) + dot(weights.astype(jnp.bfloat16), high)
        own_ref[rows] = grad_kv[:BLOCK]
        for n in range(LEVELS * PER):
            at = pl.ds(places[n], BLOCK)
            sums[n // PER, at, :] += grad_kv[(n + 1) * BLOCK : (n + 2) * BLOCK]
        grad_q = dot(dscores, kv, TN) * DH ** (-0.5)
        for pair in range(heads // 2):
            first = grad_q[2 * pair * BLOCK : (2 * pair + 1) * BLOCK]
            second = grad_q[(2 * pair + 1) * BLOCK : (2 * pair + 2) * BLOCK]
            both = jnp.where(lane < DH, first, pltpu.roll(second, DH, 1)).astype(gq_ref.dtype)
            gq_ref[rows, pair * 2 * DH : (pair + 1) * 2 * DH] = both
            gq_too_ref[rows, pair * 2 * DH : (pair + 1) * 2 * DH] = both
    for level in range(LEVELS):
        back_refs[level][...] = sums[level].astype(jnp.bfloat16)


def attention(distances, chosen, q, go, ao, lse, kv, far):
    tokens, width = q.shape
    shape = (jax.ShapeDtypeStruct((tokens, width), jnp.bfloat16),) * 2
    shape += (jax.ShapeDtypeStruct(kv.shape, jnp.float32),)
    shape += (jax.ShapeDtypeStruct(kv.shape, jnp.bfloat16),) * LEVELS
    return call(
        functools.partial(attention_kernel, distances),
        2 * 10**9,
        shape,
        chosen,
        q,
        go,
        ao,
        lse,
        kv,
        *far,
        smem=1,
        scratch=[pltpu.VMEM((LEVELS, *kv.shape), jnp.float32), pltpu.VMEM(kv.shape, kv.dtype)],
    )


def weight_kernel(mine_ref, other_ref, x_ref, out_ref):
    core = lax.axis_index("c")
    peers = x_ref.shape[0] // 2
    ys = out_ref.shape[0]
    grads = jnp.concatenate([mine_ref[...], other_ref[...]], axis=0)
    for peer in range(peers):
        x = jnp.concatenate(
            [x_ref[core * peers + peer], x_ref[(1 - core) * peers + peer]], axis=0
        )
        part = dot(x, grads, TN).astype(out_ref.dtype)
        step = part.shape[0] // ys
        for y in range(ys):
            out_ref[y, peer * step : (peer + 1) * step] = part[y * step : (y + 1) * step]


def weight(mine, other, x, ys):
    peers, tokens, part = x.shape[0] // 2, x.shape[1], x.shape[2]
    shape = jax.ShapeDtypeStruct((ys, peers * part // ys, mine.shape[1]), jnp.bfloat16)
    flops = 4 * tokens * peers * part * mine.shape[1]
    return call(weight_kernel, flops, shape, mine, other, x)


def sum_kernel(tiles_ref, out_ref):
    total = tiles_ref[0].astype(jnp.float32)
    for n in range(1, tiles_ref.shape[0]):
        total = total + tiles_ref[n].astype(jnp.float32)
    out_ref[...] = total.astype(out_ref.dtype)


def summed(tiles, dtype):
    shape = jax.ShapeDtypeStruct(tiles.shape[1:], dtype)
    return call(sum_kernel, tiles.size, shape, tiles)


def collect_kernel(own_ref, *refs):
    total = own_ref[...]
    for ref in refs[:LEVELS]:
        total = total + ref[...].astype(jnp.float32)
    total = turned(total)
    width = total.shape[0] // 2
    refs[LEVELS][...] = total[:width].astype(jnp.bfloat16)
    refs[LEVELS + 1][...] = total[width:].astype(jnp.bfloat16)


def collect(own, back):
    shape = jax.ShapeDtypeStruct((own.shape[1] // 2, own.shape[0]), jnp.bfloat16)
    return call(collect_kernel, 10**6, (shape, shape), own, *back)


def shards(layer_input, queries, keys, values, attn_out, grad_out, log_sum, chosen):
    axis_size = lax.axis_size(KV)
    ys, cores, peers = lax.axis_size("y"), lax.axis_size("c"), lax.axis_size("x")
    out_rows = layer_input.shape[1] * peers // axis_size
    distances = [1, axis_size // 8, axis_size // 4, axis_size // 2]
    key_pair = pack(keys.T, values.T)
    far = []
    for distance in distances[:2]:
        far.append(shifted(key_pair, KV, distance))
    quarter = lax.axis_size("z") // 4
    quarters = [range(n * quarter, (n + 1) * quarter) for n in range(4)]
    traded = between(key_pair, quarters, ((0, 1), (1, 0)))
    passed = between(traded, quarters, ((1, 2), (0, 3)))
    fetched = between(key_pair, quarters, ((1, 2), (2, 3)))
    far += [traded, fetched, passed]
    sent = spread(layer_input, out_rows, ys, cores, peers)
    whole_input = exchanged(sent, ("c", "x"))
    grad_queries, grads, own, *back = attention(
        distances, chosen.T, queries, grad_out, attn_out, log_sum.T, key_pair, far
    )
    route = [(i, cores - 1 - i) for i in range(cores)]
    other = lax.ppermute(grads, "c", route)
    parts = weight(grads, other, whole_input, ys)
    over_y = exchanged(parts, "y")
    returned = []
    for level, distance in enumerate(distances):
        returned.append(shifted(back[level], KV, -distance))
    over_y = summed(over_y.reshape(ys, -1, out_rows, over_y.shape[2]), jnp.bfloat16)
    over_z = exchanged(over_y, "z")
    grad_keys, grad_values = collect(own, returned)
    grad_weight = summed(over_z, jnp.float32)
    return (grad_queries, grad_keys.T, grad_values.T, grad_weight)


def solution(mesh):
    ys, cores = SIDES
    shape = (mesh.shape["kv"] // (ys * cores), ys, cores, mesh.shape["tp"])
    torus = Mesh(mesh.devices.reshape(shape), (*KV, "x"))
    return jax.shard_map(
        shards,
        mesh=torus,
        in_specs=(P(KV, "x"),) * 7 + (P(),),
        out_specs=(P(KV, "x"),) * 4,
        check_vma=False,
    )
```

```python
import functools

import jax
import jax.numpy as jnp
from jax import lax
from jax.experimental import pallas as pl
from jax.experimental.pallas import tpu as pltpu
from jax.sharding import Mesh
from jax.sharding import PartitionSpec as P

DH = 64
BLOCK = 64
PER = 2
LEVELS = 4
SIDES = (8, 2)
KV = ("z", "y", "c")
NT = (((1,), (1,)), ((), ()))
TN = (((0,), (0,)), ((), ()))
Y_ORDERS = ((4, 5, 6, 7, 0, 1, 2, 3), (3, 2, 1, 0, 7, 6, 5, 4))
VMEM_LIMIT = 16 * 2**20


def shifted(block, axis, distance):
    devices = range(lax.axis_size(axis))
    route = [(i - distance, i) for i in devices if i - distance in devices]
    return lax.ppermute(block, axis, route)


def between(block, quarters, pairs):
    route = [p for a, b in pairs for p in zip(quarters[a], quarters[b])]
    return lax.ppermute(block, "z", route)


def exchanged(tiles, axis, groups=None):
    return lax.all_to_all(
        tiles, axis, split_axis=0, concat_axis=0, tiled=True, axis_index_groups=groups
    )


def dot(a, b, dims=(((1,), (0,)), ((), ()))):
    return lax.dot_general(a, b, dims, preferred_element_type=jnp.float32)


def call(kernel, flops, out_shape, *args, smem=0, scratch=()):
    vmem = pl.BlockSpec(memory_space=pltpu.VMEM)
    many = isinstance(out_shape, tuple)
    size = sum(a.size * a.dtype.itemsize for a in args)
    return pl.pallas_call(
        kernel,
        out_shape=out_shape,
        in_specs=[pl.BlockSpec(memory_space=pltpu.SMEM)] * smem + [vmem] * (len(args) - smem),
        out_specs=(vmem,) * len(out_shape) if many else vmem,
        scratch_shapes=scratch,
        cost_estimate=pl.CostEstimate(flops=flops, bytes_accessed=size, transcendentals=0),
        compiler_params=pltpu.CompilerParams(vmem_limit_bytes=VMEM_LIMIT),
    )(*args)


def turned(x):
    return jnp.transpose(x.astype(jnp.float32))


def pack_kernel(kv_ref, out_ref):
    out_ref[...] = turned(kv_ref[...]).astype(out_ref.dtype)


def pack(k, v):
    kv = jnp.concatenate([k, v], axis=0)
    shape = jax.ShapeDtypeStruct(kv.shape[::-1], kv.dtype)
    return call(pack_kernel, 10**10, shape, kv)


def spread_kernel(rows, ys, cores, peers, x_ref, out_ref):
    width = x_ref.shape[1]
    source = lax.broadcasted_iota(jnp.int32, (width, 1), 0)
    target = lax.broadcasted_iota(jnp.int32, (width, width), 1)
    inner, left = source & (rows - 1), source // rows
    core, left = left & (cores - 1), left // cores
    y, z = left & (ys - 1), left // ys
    zs = width // (rows * cores * ys)
    place = ((core * ys + y) * zs + z) * rows + inner
    move = jnp.where(place == target, 1.0, 0.0).astype(jnp.bfloat16)
    moved = dot(x_ref[...], move).astype(jnp.bfloat16)
    part = width // cores
    for core in range(cores):
        for peer in range(peers):
            out_ref[core * peers + peer] = moved[:, core * part : (core + 1) * part]


def spread(x, rows, ys, cores, peers):
    tokens, width = x.shape
    kernel = functools.partial(spread_kernel, rows, ys, cores, peers)
    shape = jax.ShapeDtypeStruct((cores * peers, tokens, width // cores), x.dtype)
    return call(kernel, 2 * tokens * width * width, shape, x)


def stacked(block, at):
    block = block.astype(jnp.float32)
    lane = lax.broadcasted_iota(jnp.int32, (BLOCK, 2 * DH), 1)
    keep = (lane >= at) & (lane < at + DH)
    parts = []
    for head in range(block.shape[1] // DH):
        pair = block[:, (head // 2) * 2 * DH : (head // 2 + 1) * 2 * DH]
        if (head % 2) * DH != at:
            pair = pltpu.roll(pair, DH, 1)
        parts.append(jnp.where(keep, pair, 0.0))
    return jnp.concatenate(parts, axis=0)


def row_sums(terms, pieces):
    ones = jnp.ones((8, terms.shape[1]), jnp.bfloat16)
    total = None
    for _ in range(pieces):
        piece = terms.astype(jnp.bfloat16)
        terms = terms - piece.astype(jnp.float32)
        part = dot(ones, piece, NT)
        total = part if total is None else total + part
    return total[:1]


def attention_kernel(distances, chosen_ref, q_ref, go_ref, ao_ref, lse_ref, kv_ref, *refs):
    one_ref, two_ref, traded_ref, fetched_ref, passed_ref = refs[: LEVELS + 1]
    gq_ref, gq_too_ref, own_ref = refs[LEVELS + 1 : LEVELS + 4]
    back_refs = refs[LEVELS + 4 : 2 * LEVELS + 4]
    sums, four_ref = refs[2 * LEVELS + 4 :]
    at, quarter = lax.axis_index("z"), lax.axis_size("z") // 4
    in_second = jnp.logical_and(at >= quarter, at < 2 * quarter)
    four_ref[...] = jnp.where(in_second, traded_ref[...], fetched_ref[...])
    far_refs = (one_ref, two_ref, four_ref, passed_ref)
    blocks = q_ref.shape[0] // BLOCK
    heads = q_ref.shape[1] // DH
    me = lax.axis_index(KV)
    lane = lax.broadcasted_iota(jnp.int32, (BLOCK, 2 * DH), 1)
    sums[...] = jnp.zeros_like(sums)
    key_at = lax.broadcasted_iota(jnp.int32, (BLOCK, heads * BLOCK), 0)
    query_at = lax.broadcasted_iota(jnp.int32, (BLOCK, heads * BLOCK), 1) & (BLOCK - 1)
    causal = key_at <= query_at
    for b in range(blocks):
        rows = slice(b * BLOCK, (b + 1) * BLOCK)
        low = stacked(q_ref[rows] * DH ** (-0.5), 0)
        high = stacked(go_ref[rows], DH)
        delta = row_sums(high * stacked(ao_ref[rows], DH), 2)
        lse = jnp.concatenate([lse_ref[h : h + 1, rows] for h in range(heads)], axis=1)
        low = low.astype(jnp.bfloat16)
        high = high.astype(jnp.bfloat16)
        places = []
        for n in range(LEVELS * PER):
            block = chosen_ref[n, me * blocks + b]
            block = jnp.where(block >= 0, block - (me - distances[n // PER]) * blocks, 0)
            places.append(pl.multiple_of(block * BLOCK, BLOCK))
        kv = jnp.concatenate(
            [kv_ref[rows]]
            + [far_refs[n // PER][pl.ds(places[n], BLOCK), :] for n in range(LEVELS * PER)],
            axis=0,
        )
        weights = jnp.exp(dot(kv, low, NT) - lse)
        weights = jnp.concatenate(
            [jnp.where(causal, weights[:BLOCK], 0.0), weights[BLOCK:]], axis=0
        )
        dscores = (weights * (dot(kv, high, NT) - delta)).astype(jnp.bfloat16)
        grad_kv = dot(dscores, low) + dot(weights.astype(jnp.bfloat16), high)
        own_ref[rows] = grad_kv[:BLOCK]
        for n in range(LEVELS * PER):
            at = pl.ds(places[n], BLOCK)
            sums[n // PER, at, :] += grad_kv[(n + 1) * BLOCK : (n + 2) * BLOCK]
        grad_q = dot(dscores, kv, TN) * DH ** (-0.5)
        for pair in range(heads // 2):
            first = grad_q[2 * pair * BLOCK : (2 * pair + 1) * BLOCK]
            second = grad_q[(2 * pair + 1) * BLOCK : (2 * pair + 2) * BLOCK]
            both = jnp.where(lane < DH, first, pltpu.roll(second, DH, 1)).astype(gq_ref.dtype)
            gq_ref[rows, pair * 2 * DH : (pair + 1) * 2 * DH] = both
            gq_too_ref[rows, pair * 2 * DH : (pair + 1) * 2 * DH] = both
    for level in range(LEVELS):
        back_refs[level][...] = sums[level].astype(jnp.bfloat16)


def attention(distances, chosen, q, go, ao, lse, kv, far):
    tokens, width = q.shape
    shape = (jax.ShapeDtypeStruct((tokens, width), jnp.bfloat16),) * 2
    shape += (jax.ShapeDtypeStruct(kv.shape, jnp.float32),)
    shape += (jax.ShapeDtypeStruct(kv.shape, jnp.bfloat16),) * LEVELS
    return call(
        functools.partial(attention_kernel, distances),
        2 * 10**9,
        shape,
        chosen,
        q,
        go,
        ao,
        lse,
        kv,
        *far,
        smem=1,
        scratch=[pltpu.VMEM((LEVELS, *kv.shape), jnp.float32), pltpu.VMEM(kv.shape, kv.dtype)],
    )


def weight_kernel(mine_ref, other_ref, x_ref, out_ref):
    core = lax.axis_index("c")
    peers = x_ref.shape[0] // 2
    ys = out_ref.shape[0]
    grads = jnp.concatenate([mine_ref[...], other_ref[...]], axis=0)
    for peer in range(peers):
        x = jnp.concatenate(
            [x_ref[core * peers + peer], x_ref[(1 - core) * peers + peer]], axis=0
        )
        part = dot(x, grads, TN).astype(out_ref.dtype)
        step = part.shape[0] // ys
        for y in range(ys):
            slot = jnp.where(core == 0, *(order.index(y) for order in Y_ORDERS))
            out_ref[slot, peer * step : (peer + 1) * step] = part[y * step : (y + 1) * step]


def weight(mine, other, x, ys):
    peers, tokens, part = x.shape[0] // 2, x.shape[1], x.shape[2]
    shape = jax.ShapeDtypeStruct((ys, peers * part // ys, mine.shape[1]), jnp.bfloat16)
    flops = 4 * tokens * peers * part * mine.shape[1]
    return call(weight_kernel, flops, shape, mine, other, x)


def sum_kernel(tiles_ref, out_ref):
    total = tiles_ref[0].astype(jnp.float32)
    for n in range(1, tiles_ref.shape[0]):
        total = total + tiles_ref[n].astype(jnp.float32)
    out_ref[...] = total.astype(out_ref.dtype)


def summed(tiles, dtype):
    shape = jax.ShapeDtypeStruct(tiles.shape[1:], dtype)
    return call(sum_kernel, tiles.size, shape, tiles)


def collect_kernel(own_ref, *refs):
    total = own_ref[...]
    for ref in refs[:LEVELS]:
        total = total + ref[...].astype(jnp.float32)
    total = turned(total)
    width = total.shape[0] // 2
    refs[LEVELS][...] = total[:width].astype(jnp.bfloat16)
    refs[LEVELS + 1][...] = total[width:].astype(jnp.bfloat16)


def collect(own, back):
    shape = jax.ShapeDtypeStruct((own.shape[1] // 2, own.shape[0]), jnp.bfloat16)
    return call(collect_kernel, 10**6, (shape, shape), own, *back)


def shards(layer_input, queries, keys, values, attn_out, grad_out, log_sum, chosen):
    axis_size = lax.axis_size(KV)
    ys, cores, peers = lax.axis_size("y"), lax.axis_size("c"), lax.axis_size("x")
    out_rows = layer_input.shape[1] * peers // axis_size
    distances = [1, axis_size // 8, axis_size // 4, axis_size // 2]
    key_pair = pack(keys.T, values.T)
    far = []
    for distance in distances[:2]:
        far.append(shifted(key_pair, KV, distance))
    quarter = lax.axis_size("z") // 4
    quarters = [range(n * quarter, (n + 1) * quarter) for n in range(4)]
    traded = between(key_pair, quarters, ((0, 1), (1, 0)))
    passed = between(traded, quarters, ((1, 2), (0, 3)))
    fetched = between(key_pair, quarters, ((1, 2), (2, 3)))
    far += [traded, fetched, passed]
    sent = spread(layer_input, out_rows, ys, cores, peers)
    whole_input = exchanged(sent, ("c", "x"))
    grad_queries, grads, own, *back = attention(
        distances, chosen.T, queries, grad_out, attn_out, log_sum.T, key_pair, far
    )
    route = [(i, cores - 1 - i) for i in range(cores)]
    other = lax.ppermute(grads, "c", route)
    parts = weight(grads, other, whole_input, ys)
    groups = [[y * cores + c for y in order] for c, order in enumerate(Y_ORDERS)]
    over_y = exchanged(parts, ("y", "c"), groups)
    returned = []
    for level, distance in enumerate(distances):
        returned.append(shifted(back[level], KV, -distance))
    over_y = summed(over_y.reshape(ys, -1, out_rows, over_y.shape[2]), jnp.bfloat16)
    over_z = exchanged(over_y, "z")
    grad_keys, grad_values = collect(own, returned)
    grad_weight = summed(over_z, jnp.float32)
    return (grad_queries, grad_keys.T, grad_values.T, grad_weight)


def solution(mesh):
    ys, cores = SIDES
    shape = (mesh.shape["kv"] // (ys * cores), ys, cores, mesh.shape["tp"])
    torus = Mesh(mesh.devices.reshape(shape), (*KV, "x"))
    return jax.shard_map(
        shards,
        mesh=torus,
        in_specs=(P(KV, "x"),) * 7 + (P(),),
        out_specs=(P(KV, "x"),) * 4,
        check_vma=False,
    )
```

```python
import functools

import jax
import jax.numpy as jnp
from jax import lax
from jax.experimental import pallas as pl
from jax.experimental.pallas import tpu as pltpu
from jax.sharding import Mesh
from jax.sharding import PartitionSpec as P

DH = 64
BLOCK = 64
PER = 2
LEVELS = 4
SIDES = (8, 2)
KV = ("z", "y", "c")
NT = (((1,), (1,)), ((), ()))
TN = (((0,), (0,)), ((), ()))
Y_ORDERS = ((4, 5, 6, 7, 0, 1, 2, 3), (3, 2, 1, 0, 7, 6, 5, 4))
Z_ORDER = (8, 9, 10, 11, 12, 13, 14, 15, 0, 1, 2, 3, 4, 5, 6, 7)
LANES = 128
VMEM_LIMIT = 16 * 2**20


def shifted(block, axis, distance, senders=None, receivers=None):
    devices = range(lax.axis_size(axis))
    senders, receivers = senders or devices, receivers or devices
    route = [(i, i + distance) for i in senders if i + distance in receivers]
    return lax.ppermute(block, axis, route)


def between(block, quarters, pairs):
    route = [p for a, b in pairs for p in zip(quarters[a], quarters[b])]
    return lax.ppermute(block, "z", route)


def exchanged(tiles, axis, groups=None):
    return lax.all_to_all(
        tiles, axis, split_axis=0, concat_axis=0, tiled=True, axis_index_groups=groups
    )


def dot(a, b, dims=(((1,), (0,)), ((), ()))):
    return lax.dot_general(a, b, dims, preferred_element_type=jnp.float32)


def call(kernel, flops, out_shape, *args, smem=0, scratch=()):
    vmem = pl.BlockSpec(memory_space=pltpu.VMEM)
    many = isinstance(out_shape, tuple)
    size = sum(a.size * a.dtype.itemsize for a in args)
    return pl.pallas_call(
        kernel,
        out_shape=out_shape,
        in_specs=[pl.BlockSpec(memory_space=pltpu.SMEM)] * smem + [vmem] * (len(args) - smem),
        out_specs=(vmem,) * len(out_shape) if many else vmem,
        scratch_shapes=scratch,
        cost_estimate=pl.CostEstimate(flops=flops, bytes_accessed=size, transcendentals=0),
        compiler_params=pltpu.CompilerParams(vmem_limit_bytes=VMEM_LIMIT),
    )(*args)


def turned(x):
    return jnp.transpose(x.astype(jnp.float32))


def pack_kernel(kv_ref, out_ref):
    out_ref[...] = turned(kv_ref[...]).astype(out_ref.dtype)


def pack(k, v):
    kv = jnp.concatenate([k, v], axis=0)
    shape = jax.ShapeDtypeStruct(kv.shape[::-1], kv.dtype)
    return call(pack_kernel, 10**10, shape, kv)


def spread_kernel(rows, ys, cores, peers, x_ref, out_ref, held, done):
    width = x_ref.shape[1]
    source = lax.broadcasted_iota(jnp.int32, (width, 1), 0)
    target = lax.broadcasted_iota(jnp.int32, (width, width), 1)
    inner, left = source & (rows - 1), source // rows
    core, left = left & (cores - 1), left // cores
    y, z = left & (ys - 1), left // ys
    zs = width // (rows * cores * ys)
    place = ((core * ys + y) * zs + z) * rows + inner
    move = jnp.where(place == target, 1.0, 0.0).astype(jnp.bfloat16)
    moved = dot(x_ref[...], move).astype(jnp.bfloat16)
    part = width // cores
    copies = []
    for core in range(cores):
        held[core] = moved[:, core * part : (core + 1) * part]
        for peer in range(peers):
            slot = core * peers + peer
            copies.append(pltpu.make_async_copy(held.at[core], out_ref.at[slot], done.at[slot]))
            copies[-1].start()
    for copy in copies:
        copy.wait()


def spread(x, rows, ys, cores, peers):
    tokens, width = x.shape
    part = (tokens, width // cores)
    return pl.pallas_call(
        functools.partial(spread_kernel, rows, ys, cores, peers),
        out_shape=jax.ShapeDtypeStruct((cores * peers, *part), x.dtype),
        in_specs=[pl.BlockSpec(memory_space=pltpu.VMEM)],
        out_specs=pl.BlockSpec(memory_space=pltpu.HBM),
        scratch_shapes=[
            pltpu.VMEM((cores, *part), x.dtype),
            pltpu.SemaphoreType.DMA((cores * peers,)),
        ],
        cost_estimate=pl.CostEstimate(
            flops=2 * tokens * width * width, bytes_accessed=10**6, transcendentals=0
        ),
        compiler_params=pltpu.CompilerParams(vmem_limit_bytes=VMEM_LIMIT),
        name="spread",
    )(x)


def stacked(block, at):
    block = block.astype(jnp.float32)
    lane = lax.broadcasted_iota(jnp.int32, (BLOCK, 2 * DH), 1)
    keep = (lane >= at) & (lane < at + DH)
    parts = []
    for head in range(block.shape[1] // DH):
        pair = block[:, (head // 2) * 2 * DH : (head // 2 + 1) * 2 * DH]
        if (head % 2) * DH != at:
            pair = pltpu.roll(pair, DH, 1)
        parts.append(jnp.where(keep, pair, 0.0))
    return jnp.concatenate(parts, axis=0)


def row_sums(terms, pieces):
    ones = jnp.ones((8, terms.shape[1]), jnp.bfloat16)
    total = None
    for _ in range(pieces):
        piece = terms.astype(jnp.bfloat16)
        terms = terms - piece.astype(jnp.float32)
        part = dot(ones, piece, NT)
        total = part if total is None else total + part
    return total[:1]


def attention_kernel(distances, chosen_ref, q_ref, go_ref, ao_ref, lse_ref, kv_ref, *refs):
    one_ref, *step_refs, traded_ref, fetched_ref, passed_ref = refs[: LEVELS + 2]
    gq_ref, own_ref = refs[LEVELS + 2 : LEVELS + 4]
    back_refs = refs[LEVELS + 4 : 2 * LEVELS + 4]
    sums, two_ref, four_ref, table, done = refs[2 * LEVELS + 4 :]
    blocks = q_ref.shape[0] // BLOCK
    heads = q_ref.shape[1] // DH
    me = lax.axis_index(KV)
    width = table.shape[1]
    start = jnp.minimum(me * blocks // LANES * LANES, chosen_ref.shape[1] - width)
    start = pl.multiple_of(start, LANES)
    copy = pltpu.make_async_copy(chosen_ref.at[:, pl.ds(start, width)], table, done)
    copy.start()
    at, quarter = lax.axis_index("z"), lax.axis_size("z") // 4
    in_second = jnp.logical_and(at >= quarter, at < 2 * quarter)
    is_late = me - distances[1] >= lax.axis_size(KV) // 2
    two_ref[...] = jnp.where(is_late, step_refs[1][...], step_refs[0][...])
    four_ref[...] = jnp.where(in_second, traded_ref[...], fetched_ref[...])
    far_refs = (one_ref, two_ref, four_ref, passed_ref)
    lane = lax.broadcasted_iota(jnp.int32, (BLOCK, 2 * DH), 1)
    key_at = lax.broadcasted_iota(jnp.int32, (BLOCK, heads * BLOCK), 0)
    query_at = lax.broadcasted_iota(jnp.int32, (BLOCK, heads * BLOCK), 1) & (BLOCK - 1)
    causal = key_at <= query_at
    sums[...] = jnp.zeros_like(sums)
    staged = []
    for b in range(blocks):
        rows = slice(b * BLOCK, (b + 1) * BLOCK)
        low = stacked(q_ref[rows] * DH ** (-0.5), 0)
        high = stacked(go_ref[rows], DH)
        delta = row_sums(high * stacked(ao_ref[rows], DH), 2)
        lse = jnp.concatenate([lse_ref[h : h + 1, rows] for h in range(heads)], axis=1)
        staged.append((low.astype(jnp.bfloat16), high.astype(jnp.bfloat16), lse, delta))
    copy.wait()
    for b, (low, high, lse, delta) in enumerate(staged):
        rows = slice(b * BLOCK, (b + 1) * BLOCK)
        places = []
        for n in range(LEVELS * PER):
            block = table[n, me * blocks - start + b]
            block = jnp.where(block >= 0, block - (me - distances[n // PER]) * blocks, 0)
            places.append(pl.multiple_of(block * BLOCK, BLOCK))
        kv = jnp.concatenate(
            [kv_ref[rows]]
            + [far_refs[n // PER][pl.ds(places[n], BLOCK), :] for n in range(LEVELS * PER)],
            axis=0,
        )
        weights = jnp.exp(dot(kv, low, NT) - lse)
        weights = jnp.concatenate(
            [jnp.where(causal, weights[:BLOCK], 0.0), weights[BLOCK:]], axis=0
        )
        dscores = (weights * (dot(kv, high, NT) - delta)).astype(jnp.bfloat16)
        grad_kv = dot(dscores, low) + dot(weights.astype(jnp.bfloat16), high)
        own_ref[rows] = grad_kv[:BLOCK]
        for n in range(LEVELS * PER):
            at = pl.ds(places[n], BLOCK)
            sums[n // PER, at, :] += grad_kv[(n + 1) * BLOCK : (n + 2) * BLOCK]
        grad_q = dot(dscores, kv, TN) * DH ** (-0.5)
        for pair in range(heads // 2):
            first = grad_q[2 * pair * BLOCK : (2 * pair + 1) * BLOCK]
            second = grad_q[(2 * pair + 1) * BLOCK : (2 * pair + 2) * BLOCK]
            gq_ref[rows, pair * 2 * DH : (pair + 1) * 2 * DH] = jnp.where(
                lane < DH, first, pltpu.roll(second, DH, 1)
            ).astype(gq_ref.dtype)
    for level in range(LEVELS):
        back_refs[level][...] = sums[level].astype(jnp.bfloat16)


def attention(distances, chosen, q, go, ao, lse, kv, far):
    tokens, width = q.shape
    shape = (jax.ShapeDtypeStruct((tokens, width), jnp.bfloat16),)
    shape += (jax.ShapeDtypeStruct(kv.shape, jnp.float32),)
    shape += (jax.ShapeDtypeStruct(kv.shape, jnp.bfloat16),) * LEVELS
    return call(
        functools.partial(attention_kernel, distances),
        2 * 10**9,
        shape,
        chosen,
        q,
        go,
        ao,
        lse,
        kv,
        *far,
        scratch=[
            pltpu.VMEM((LEVELS, *kv.shape), jnp.float32),
            pltpu.VMEM(kv.shape, kv.dtype),
            pltpu.VMEM(kv.shape, kv.dtype),
            pltpu.SMEM((chosen.shape[0], min(2 * LANES, chosen.shape[1])), chosen.dtype),
            pltpu.SemaphoreType.DMA,
        ],
    )


def weight_kernel(mine_ref, other_ref, x_ref, out_ref):
    core = lax.axis_index("c")
    peers = x_ref.shape[0] // 2
    ys = out_ref.shape[0]
    grads = jnp.concatenate([mine_ref[...], other_ref[...]], axis=0)
    for peer in range(peers):
        x = jnp.concatenate(
            [x_ref[core * peers + peer], x_ref[(1 - core) * peers + peer]], axis=0
        )
        part = dot(x, grads, TN).astype(out_ref.dtype)
        step = part.shape[0] // ys
        for y in range(ys):
            slot = jnp.where(core == 0, *(order.index(y) for order in Y_ORDERS))
            out_ref[slot, peer * step : (peer + 1) * step] = part[y * step : (y + 1) * step]


def weight(mine, other, x, ys):
    peers, tokens, part = x.shape[0] // 2, x.shape[1], x.shape[2]
    shape = jax.ShapeDtypeStruct((ys, peers * part // ys, mine.shape[1]), jnp.bfloat16)
    flops = 4 * tokens * peers * part * mine.shape[1]
    return call(weight_kernel, flops, shape, mine, other, x)


def sum_kernel(order, tiles_ref, out_ref):
    total = tiles_ref[0].astype(jnp.float32)
    for n in range(1, tiles_ref.shape[0]):
        total = total + tiles_ref[n].astype(jnp.float32)
    total = total.astype(out_ref.dtype)
    if order is None:
        out_ref[...] = total
    else:
        for slot, place in enumerate(order):
            out_ref[slot] = total[place]


def summed(tiles, dtype, order=None):
    shape = jax.ShapeDtypeStruct(tiles.shape[1:], dtype)
    return call(functools.partial(sum_kernel, order), tiles.size, shape, tiles)


def collect_kernel(grads_ref, own_ref, *refs):
    *parts, gq_ref, gk_ref, gv_ref = refs
    total = own_ref[...]
    for ref in parts:
        total = total + ref[...].astype(jnp.float32)
    total = turned(total)
    width = total.shape[0] // 2
    gq_ref[...] = grads_ref[...]
    gk_ref[...] = total[:width].astype(jnp.bfloat16)
    gv_ref[...] = total[width:].astype(jnp.bfloat16)


def collect(grads, own, back):
    shape = jax.ShapeDtypeStruct((own.shape[1] // 2, own.shape[0]), jnp.bfloat16)
    shapes = (jax.ShapeDtypeStruct(grads.shape, grads.dtype), shape, shape)
    return call(collect_kernel, 10**6, shapes, grads, own, *back)


def shards(layer_input, queries, keys, values, attn_out, grad_out, log_sum, chosen):
    axis_size = lax.axis_size(KV)
    ys, cores, peers = lax.axis_size("y"), lax.axis_size("c"), lax.axis_size("x")
    out_rows = layer_input.shape[1] * peers // axis_size
    distances = [1, axis_size // 8, axis_size // 4, axis_size // 2]
    key_pair = pack(keys.T, values.T)
    near = shifted(key_pair, KV, distances[0])
    halves = [range(axis_size // 2), range(axis_size // 2, axis_size)]
    steps = []
    for senders in halves:
        steps.append(shifted(key_pair, KV, distances[1], senders))
    quarter = lax.axis_size("z") // 4
    quarters = [range(n * quarter, (n + 1) * quarter) for n in range(4)]
    traded = between(key_pair, quarters, ((0, 1), (1, 0)))
    passed = between(traded, quarters, ((1, 2), (0, 3)))
    fetched = between(key_pair, quarters, ((1, 2), (2, 3)))
    far = [near, *steps, traded, fetched, passed]
    sent = spread(layer_input, out_rows, ys, cores, peers)
    whole_input = exchanged(sent, ("c", "x"))
    grads, own, *back = attention(
        distances, chosen.T, queries, grad_out, attn_out, log_sum.T, key_pair, far
    )
    route = [(i, cores - 1 - i) for i in range(cores)]
    other = lax.ppermute(grads, "c", route)
    parts = weight(grads, other, whole_input, ys)
    groups = [[y * cores + c for y in order] for c, order in enumerate(Y_ORDERS)]
    over_y = exchanged(parts, ("y", "c"), groups)
    returned = []
    for level, distance in enumerate(distances[:-1]):
        for receivers in halves:
            block = shifted(back[level], KV, -distance, receivers=receivers)
            returned.append(block)
    returned.append(shifted(back[-1], KV, -distances[-1]))
    over_y = summed(over_y.reshape(ys, -1, out_rows, over_y.shape[2]), jnp.bfloat16, Z_ORDER)
    over_z = exchanged(over_y, "z", [list(Z_ORDER)])
    grad_queries, grad_keys, grad_values = collect(grads, own, returned)
    grad_weight = summed(over_z, jnp.float32)
    return (grad_queries, grad_keys.T, grad_values.T, grad_weight)


def solution(mesh):
    ys, cores = SIDES
    shape = (mesh.shape["kv"] // (ys * cores), ys, cores, mesh.shape["tp"])
    torus = Mesh(mesh.devices.reshape(shape), (*KV, "x"))
    return jax.shard_map(
        shards,
        mesh=torus,
        in_specs=(P(KV, "x"),) * 7 + (P(),),
        out_specs=(P(KV, "x"),) * 4,
        check_vma=False,
    )
```

```python
import functools

import jax
import jax.numpy as jnp
from jax import lax
from jax.experimental import pallas as pl
from jax.experimental.pallas import tpu as pltpu
from jax.sharding import Mesh
from jax.sharding import PartitionSpec as P

DH = 64
BLOCK = 64
PER = 2
LEVELS = 4
SIDES = (8, 2)
KV = ("z", "y", "c")
NT = (((1,), (1,)), ((), ()))
TN = (((0,), (0,)), ((), ()))
Y_ORDERS = ((3, 2, 1, 0, 7, 6, 5, 4), (5, 6, 7, 0, 1, 2, 3, 4))
Z_ORDER = (8, 9, 10, 11, 12, 13, 14, 15, 0, 1, 2, 3, 4, 5, 6, 7)
LANES = 128
WINDOWS = 2
VMEM_LIMIT = 16 * 2**20


def shifted(block, axis, distance, senders=None, receivers=None):
    devices = range(lax.axis_size(axis))
    senders, receivers = senders or devices, receivers or devices
    route = [(i, i + distance) for i in senders if i + distance in receivers]
    return lax.ppermute(block, axis, route)


def between(block, quarters, pairs):
    route = [p for a, b in pairs for p in zip(quarters[a], quarters[b])]
    return lax.ppermute(block, "z", route)


def exchanged(tiles, axis, groups=None):
    return lax.all_to_all(
        tiles, axis, split_axis=0, concat_axis=0, tiled=True, axis_index_groups=groups
    )


def dot(a, b, dims=(((1,), (0,)), ((), ()))):
    return lax.dot_general(a, b, dims, preferred_element_type=jnp.float32)


def call(kernel, flops, out_shape, *args, smem=0, scratch=()):
    vmem = pl.BlockSpec(memory_space=pltpu.VMEM)
    many = isinstance(out_shape, tuple)
    size = sum(a.size * a.dtype.itemsize for a in args)
    return pl.pallas_call(
        kernel,
        out_shape=out_shape,
        in_specs=[pl.BlockSpec(memory_space=pltpu.SMEM)] * smem + [vmem] * (len(args) - smem),
        out_specs=(vmem,) * len(out_shape) if many else vmem,
        scratch_shapes=scratch,
        cost_estimate=pl.CostEstimate(flops=flops, bytes_accessed=size, transcendentals=0),
        compiler_params=pltpu.CompilerParams(vmem_limit_bytes=VMEM_LIMIT),
    )(*args)


def turned(x):
    return jnp.transpose(x.astype(jnp.float32))


def pack_kernel(kv_ref, out_ref):
    out_ref[...] = turned(kv_ref[...]).astype(out_ref.dtype)


def pack(k, v):
    kv = jnp.concatenate([k, v], axis=0)
    shape = jax.ShapeDtypeStruct(kv.shape[::-1], kv.dtype)
    return call(pack_kernel, 10**10, shape, kv)


def spread_kernel(rows, ys, cores, peers, x_ref, out_ref, held, done):
    width = x_ref.shape[1]
    source = lax.broadcasted_iota(jnp.int32, (width, 1), 0)
    inner, left = source & (rows - 1), source // rows
    core, left = left & (cores - 1), left // cores
    y, z = left & (ys - 1), left // ys
    zs = width // (rows * cores * ys)
    place = ((core * ys + y) * zs + z) * rows + inner
    part = width // cores
    target = lax.broadcasted_iota(jnp.int32, (width, part), 1)
    copies = []
    for core in range(cores):
        move = jnp.where(place == target + core * part, 1.0, 0.0).astype(jnp.bfloat16)
        held[core] = dot(x_ref[...], move).astype(jnp.bfloat16)
        for peer in range(peers):
            slot = core * peers + peer
            copies.append(pltpu.make_async_copy(held.at[core], out_ref.at[slot], done.at[slot]))
            copies[-1].start()
    for copy in copies:
        copy.wait()


def spread(x, rows, ys, cores, peers):
    tokens, width = x.shape
    part = (tokens, width // cores)
    return pl.pallas_call(
        functools.partial(spread_kernel, rows, ys, cores, peers),
        out_shape=jax.ShapeDtypeStruct((cores * peers, *part), x.dtype),
        in_specs=[pl.BlockSpec(memory_space=pltpu.VMEM)],
        out_specs=pl.BlockSpec(memory_space=pltpu.HBM),
        scratch_shapes=[
            pltpu.VMEM((cores, *part), x.dtype),
            pltpu.SemaphoreType.DMA((cores * peers,)),
        ],
        cost_estimate=pl.CostEstimate(
            flops=2 * tokens * width * width, bytes_accessed=10**6, transcendentals=0
        ),
        compiler_params=pltpu.CompilerParams(vmem_limit_bytes=VMEM_LIMIT),
        name="spread",
    )(x)


def stacked(block, at):
    block = block.astype(jnp.float32)
    lane = lax.broadcasted_iota(jnp.int32, (BLOCK, 2 * DH), 1)
    keep = (lane >= at) & (lane < at + DH)
    parts = []
    for head in range(block.shape[1] // DH):
        pair = block[:, (head // 2) * 2 * DH : (head // 2 + 1) * 2 * DH]
        if (head % 2) * DH != at:
            pair = pltpu.roll(pair, DH, 1)
        parts.append(jnp.where(keep, pair, 0.0))
    return jnp.concatenate(parts, axis=0)


def row_sums(terms, pieces):
    ones = jnp.ones((8, terms.shape[1]), jnp.bfloat16)
    total = None
    for _ in range(pieces):
        piece = terms.astype(jnp.bfloat16)
        terms = terms - piece.astype(jnp.float32)
        part = dot(ones, piece, NT)
        total = part if total is None else total + part
    return total[:1]


def terms(kv, low, high, lse, delta, keep=None):
    weights = jnp.exp(dot(kv, low, NT) - lse)
    if keep is not None:
        weights = jnp.where(keep, weights, 0.0)
    dscores = (weights * (dot(kv, high, NT) - delta)).astype(jnp.bfloat16)
    grad_kv = dot(dscores, low) + dot(weights.astype(jnp.bfloat16), high)
    return dot(dscores, kv, TN), grad_kv


def own_kernel(q_ref, go_ref, ao_ref, lse_ref, kv_ref, low_ref, high_ref, rows_ref, part_ref, own_ref):
    heads = q_ref.shape[1] // DH
    key_at = lax.broadcasted_iota(jnp.int32, (BLOCK, heads * BLOCK), 0)
    query_at = lax.broadcasted_iota(jnp.int32, (BLOCK, heads * BLOCK), 1) & (BLOCK - 1)
    for b in range(q_ref.shape[0] // BLOCK):
        rows = slice(b * BLOCK, (b + 1) * BLOCK)
        low = stacked(q_ref[rows] * DH ** (-0.5), 0)
        high = stacked(go_ref[rows], DH)
        delta = row_sums(high * stacked(ao_ref[rows], DH), 2)
        lse = jnp.concatenate([lse_ref[h : h + 1, rows] for h in range(heads)], axis=1)
        low = low.astype(jnp.bfloat16)
        high = high.astype(jnp.bfloat16)
        grad_q, grad_kv = terms(kv_ref[rows], low, high, lse, delta, key_at <= query_at)
        low_ref[b] = low
        high_ref[b] = high
        rows_ref[b, :1] = lse
        rows_ref[b, 1:] = delta
        part_ref[b] = grad_q
        own_ref[rows] = grad_kv


def attend_own(q, go, ao, lse, kv):
    tokens, width = q.shape
    blocks, rows = tokens // BLOCK, width * BLOCK // DH
    shape = (jax.ShapeDtypeStruct((blocks, rows, 2 * DH), jnp.bfloat16),) * 2
    shape += (jax.ShapeDtypeStruct((blocks, 2, rows), jnp.float32),)
    shape += (jax.ShapeDtypeStruct((blocks, rows, 2 * DH), jnp.float32),)
    shape += (jax.ShapeDtypeStruct(kv.shape, jnp.float32),)
    return call(own_kernel, 10**9, shape, q, go, ao, lse, kv)


def far_kernel(distances, chosen_ref, low_ref, high_ref, rows_ref, part_ref, *refs):
    one_ref, *step_refs, traded_ref, fetched_ref, passed_ref = refs[: LEVELS + 2]
    gq_ref = refs[LEVELS + 2]
    back_refs = refs[LEVELS + 3 : 2 * LEVELS + 3]
    sums, two_ref, four_ref = refs[2 * LEVELS + 3 :]
    blocks = low_ref.shape[0]
    heads = low_ref.shape[1] // BLOCK
    me = lax.axis_index(KV)
    first = me * blocks
    start = jnp.minimum(first // LANES * LANES, chosen_ref.shape[1] - LANES * WINDOWS)
    columns = lax.broadcasted_iota(jnp.int32, (LEVELS * PER, LANES), 1)
    picked = [jnp.zeros((LEVELS * PER, LANES), jnp.int32)] * blocks
    for window in range(WINDOWS):
        tile = chosen_ref[:, pl.ds(pl.multiple_of(start + window * LANES, LANES), LANES)]
        for b in range(blocks):
            here = columns == first + b - start - window * LANES
            picked[b] = picked[b] + jnp.where(here, tile, 0)
    picked = [jnp.sum(tile.astype(jnp.float32), axis=1, keepdims=True).astype(jnp.int32) for tile in picked]
    at, quarter = lax.axis_index("z"), lax.axis_size("z") // 4
    in_second = jnp.logical_and(at >= quarter, at < 2 * quarter)
    is_late = me - distances[1] >= lax.axis_size(KV) // 2
    two_ref[...] = jnp.where(is_late, step_refs[1][...], step_refs[0][...])
    four_ref[...] = jnp.where(in_second, traded_ref[...], fetched_ref[...])
    far_refs = (one_ref, two_ref, four_ref, passed_ref)
    lane = lax.broadcasted_iota(jnp.int32, (BLOCK, 2 * DH), 1)
    sums[...] = jnp.zeros_like(sums)
    for b in range(blocks):
        rows = slice(b * BLOCK, (b + 1) * BLOCK)
        places = []
        for n in range(LEVELS * PER):
            block = picked[b][n, 0]
            block = jnp.where(block >= 0, block - (me - distances[n // PER]) * blocks, 0)
            places.append(pl.ds(pl.multiple_of(block * BLOCK, BLOCK), BLOCK))
        kv = jnp.concatenate(
            [far_refs[n // PER][places[n], :] for n in range(LEVELS * PER)], axis=0
        )
        grad_q, grad_kv = terms(
            kv, low_ref[b], high_ref[b], rows_ref[b, :1], rows_ref[b, 1:]
        )
        for n in range(LEVELS * PER):
            sums[n // PER, places[n], :] += grad_kv[n * BLOCK : (n + 1) * BLOCK]
        grad_q = (part_ref[b] + grad_q) * DH ** (-0.5)
        for pair in range(heads // 2):
            first = grad_q[2 * pair * BLOCK : (2 * pair + 1) * BLOCK]
            second = grad_q[(2 * pair + 1) * BLOCK : (2 * pair + 2) * BLOCK]
            gq_ref[rows, pair * 2 * DH : (pair + 1) * 2 * DH] = jnp.where(
                lane < DH, first, pltpu.roll(second, DH, 1)
            ).astype(gq_ref.dtype)
    for level in range(LEVELS):
        back_refs[level][...] = sums[level].astype(jnp.bfloat16)


def attend_far(distances, chosen, low, high, rows, part, far):
    tokens, width = low.shape[0] * BLOCK, low.shape[1] * DH // BLOCK
    kv = far[0]
    shape = (jax.ShapeDtypeStruct((tokens, width), jnp.bfloat16),)
    shape += (jax.ShapeDtypeStruct(kv.shape, jnp.bfloat16),) * LEVELS
    return call(
        functools.partial(far_kernel, distances),
        2 * 10**9,
        shape,
        chosen,
        low,
        high,
        rows,
        part,
        *far,
        scratch=[
            pltpu.VMEM((LEVELS, *kv.shape), jnp.float32),
            pltpu.VMEM(kv.shape, kv.dtype),
            pltpu.VMEM(kv.shape, kv.dtype),
        ],
    )


def weight_kernel(mine_ref, other_ref, x_ref, out_ref, held, done):
    core = lax.axis_index("c")
    peers = x_ref.shape[0] // 2
    ys = out_ref.shape[0]
    step = x_ref.shape[2] // ys
    grads = jnp.concatenate([mine_ref[...], other_ref[...]], axis=0)
    copies = []
    for half in range(2):
        mine = range(half * ys // 2, (half + 1) * ys // 2)
        lanes = slice(mine[0] * step, (mine[-1] + 1) * step)
        for peer in range(peers):
            x = jnp.concatenate(
                [x_ref[core * peers + peer, :, lanes], x_ref[(1 - core) * peers + peer, :, lanes]],
                axis=0,
            )
            part = dot(x, grads, TN).astype(held.dtype)
            for n, y in enumerate(mine):
                held[y, peer * step : (peer + 1) * step] = part[n * step : (n + 1) * step]
        for y in mine:
            slot = jnp.where(core == 0, *(order.index(y) for order in Y_ORDERS))
            copies.append(pltpu.make_async_copy(held.at[y], out_ref.at[slot], done.at[y]))
            copies[-1].start()
    for copy in copies:
        copy.wait()


def weight(mine, other, x, ys):
    peers, tokens, part = x.shape[0] // 2, x.shape[1], x.shape[2]
    shape = (ys, peers * part // ys, mine.shape[1])
    vmem = pl.BlockSpec(memory_space=pltpu.VMEM)
    return pl.pallas_call(
        weight_kernel,
        out_shape=jax.ShapeDtypeStruct(shape, jnp.bfloat16),
        in_specs=[vmem] * 3,
        out_specs=pl.BlockSpec(memory_space=pltpu.HBM),
        scratch_shapes=[pltpu.VMEM(shape, jnp.bfloat16), pltpu.SemaphoreType.DMA((ys,))],
        cost_estimate=pl.CostEstimate(
            flops=4 * tokens * peers * part * mine.shape[1], bytes_accessed=10**6, transcendentals=0
        ),
        compiler_params=pltpu.CompilerParams(vmem_limit_bytes=VMEM_LIMIT),
        name="weight",
    )(mine, other, x)


def sum_kernel(order, tiles_ref, out_ref):
    total = tiles_ref[0].astype(jnp.float32)
    for n in range(1, tiles_ref.shape[0]):
        total = total + tiles_ref[n].astype(jnp.float32)
    total = total.astype(out_ref.dtype)
    if order is None:
        out_ref[...] = total
    else:
        for slot, place in enumerate(order):
            out_ref[slot] = total[place]


def summed(tiles, dtype, order=None):
    shape = jax.ShapeDtypeStruct(tiles.shape[1:], dtype)
    return call(functools.partial(sum_kernel, order), tiles.size, shape, tiles)


def collect_kernel(grads_ref, own_ref, *refs):
    *parts, gq_ref, gk_ref, gv_ref = refs
    total = own_ref[...]
    for ref in parts:
        total = total + ref[...].astype(jnp.float32)
    total = turned(total)
    width = total.shape[0] // 2
    gq_ref[...] = grads_ref[...]
    gk_ref[...] = total[:width].astype(jnp.bfloat16)
    gv_ref[...] = total[width:].astype(jnp.bfloat16)


def collect(grads, own, back):
    shape = jax.ShapeDtypeStruct((own.shape[1] // 2, own.shape[0]), jnp.bfloat16)
    shapes = (jax.ShapeDtypeStruct(grads.shape, grads.dtype), shape, shape)
    return call(collect_kernel, 10**6, shapes, grads, own, *back)


def shards(layer_input, queries, keys, values, attn_out, grad_out, log_sum, chosen):
    axis_size = lax.axis_size(KV)
    ys, cores, peers = lax.axis_size("y"), lax.axis_size("c"), lax.axis_size("x")
    out_rows = layer_input.shape[1] * peers // axis_size
    distances = [1, axis_size // 8, axis_size // 4, axis_size // 2]
    key_pair = pack(keys.T, values.T)
    near = shifted(key_pair, KV, distances[0])
    halves = [range(axis_size // 2), range(axis_size // 2, axis_size)]
    steps = []
    for senders in halves:
        steps.append(shifted(key_pair, KV, distances[1], senders))
    quarter = lax.axis_size("z") // 4
    quarters = [range(n * quarter, (n + 1) * quarter) for n in range(4)]
    traded = between(key_pair, quarters, ((0, 1), (1, 0)))
    passed = between(traded, quarters, ((1, 2), (0, 3)))
    fetched = between(key_pair, quarters, ((1, 2), (2, 3)))
    far = [near, *steps, traded, fetched, passed]
    sent = spread(layer_input, out_rows, ys, cores, peers)
    whole_input = exchanged(sent, ("c", "x"))
    *staged, grad_own = attend_own(queries, grad_out, attn_out, log_sum.T, key_pair)
    grads, *back = attend_far(distances, chosen.T, *staged, far)
    route = [(i, cores - 1 - i) for i in range(cores)]
    other = lax.ppermute(grads, "c", route)
    parts = weight(grads, other, whole_input, ys)
    groups = [[y * cores + c for y in order] for c, order in enumerate(Y_ORDERS)]
    over_y = exchanged(parts, ("y", "c"), groups)
    returned = []
    for level, distance in enumerate(distances[:-1]):
        for receivers in halves:
            block = shifted(back[level], KV, -distance, receivers=receivers)
            returned.append(block)
    returned.append(shifted(back[-1], KV, -distances[-1]))
    over_y = summed(over_y.reshape(ys, -1, out_rows, over_y.shape[2]), jnp.bfloat16, Z_ORDER)
    over_z = exchanged(over_y, "z", [list(Z_ORDER)])
    grad_queries, grad_keys, grad_values = collect(grads, grad_own, returned)
    grad_weight = summed(over_z, jnp.float32)
    return (grad_queries, grad_keys.T, grad_values.T, grad_weight)


def solution(mesh):
    ys, cores = SIDES
    shape = (mesh.shape["kv"] // (ys * cores), ys, cores, mesh.shape["tp"])
    torus = Mesh(mesh.devices.reshape(shape), (*KV, "x"))
    return jax.shard_map(
        shards,
        mesh=torus,
        in_specs=(P(KV, "x"),) * 7 + (P(),),
        out_specs=(P(KV, "x"),) * 4,
        check_vma=False,
    )
```

```python
import functools

import jax
import jax.numpy as jnp
from jax import lax
from jax.experimental import pallas as pl
from jax.experimental.pallas import tpu as pltpu
from jax.sharding import Mesh
from jax.sharding import PartitionSpec as P

DH = 64
BLOCK = 64
PER = 2
LEVELS = 4
SIDES = (8, 2)
KV = ("z", "y", "c")
NT = (((1,), (1,)), ((), ()))
TN = (((0,), (0,)), ((), ()))
Y_ORDERS = ((3, 2, 1, 0, 7, 6, 5, 4), (5, 6, 7, 0, 1, 2, 3, 4))
Z_ORDER = (8, 9, 10, 11, 12, 13, 14, 15, 0, 1, 2, 3, 4, 5, 6, 7)
X_ORDER = (4, 5, 6, 7, 0, 1, 2, 3)
LANES = 128
WINDOWS = 2
VMEM_LIMIT = 16 * 2**20


def shifted(block, axis, distance, senders=None, receivers=None):
    devices = range(lax.axis_size(axis))
    senders, receivers = senders or devices, receivers or devices
    route = [(i, i + distance) for i in senders if i + distance in receivers]
    return lax.ppermute(block, axis, route)


def between(block, quarters, pairs):
    route = [p for a, b in pairs for p in zip(quarters[a], quarters[b])]
    return lax.ppermute(block, "z", route)


def exchanged(tiles, axis, groups=None):
    return lax.all_to_all(
        tiles, axis, split_axis=0, concat_axis=0, tiled=True, axis_index_groups=groups
    )


def dot(a, b, dims=(((1,), (0,)), ((), ()))):
    return lax.dot_general(a, b, dims, preferred_element_type=jnp.float32)


def call(kernel, flops, out_shape, *args, smem=0, scratch=()):
    vmem = pl.BlockSpec(memory_space=pltpu.VMEM)
    many = isinstance(out_shape, tuple)
    size = sum(a.size * a.dtype.itemsize for a in args)
    return pl.pallas_call(
        kernel,
        out_shape=out_shape,
        in_specs=[pl.BlockSpec(memory_space=pltpu.SMEM)] * smem + [vmem] * (len(args) - smem),
        out_specs=(vmem,) * len(out_shape) if many else vmem,
        scratch_shapes=scratch,
        cost_estimate=pl.CostEstimate(flops=flops, bytes_accessed=size, transcendentals=0),
        compiler_params=pltpu.CompilerParams(vmem_limit_bytes=VMEM_LIMIT),
    )(*args)


def turned(x):
    return jnp.transpose(x.astype(jnp.float32))


def pack_kernel(kv_ref, out_ref):
    out_ref[...] = turned(kv_ref[...]).astype(out_ref.dtype)


def pack(k, v):
    kv = jnp.concatenate([k, v], axis=0)
    shape = jax.ShapeDtypeStruct(kv.shape[::-1], kv.dtype)
    return call(pack_kernel, 10**10, shape, kv)


def spread_kernel(rows, ys, cores, peers, x_ref, out_ref, held, done):
    width = x_ref.shape[1]
    source = lax.broadcasted_iota(jnp.int32, (width, 1), 0)
    inner, left = source & (rows - 1), source // rows
    core, left = left & (cores - 1), left // cores
    y, z = left & (ys - 1), left // ys
    zs = width // (rows * cores * ys)
    place = ((core * ys + y) * zs + z) * rows + inner
    part = width // cores
    target = lax.broadcasted_iota(jnp.int32, (width, part), 1)
    copies = []
    for core in range(cores):
        move = jnp.where(place == target + core * part, 1.0, 0.0).astype(jnp.bfloat16)
        held[core] = dot(x_ref[...], move).astype(jnp.bfloat16)
        for peer in range(peers):
            slot = X_ORDER.index(core * peers + peer)
            copies.append(pltpu.make_async_copy(held.at[core], out_ref.at[slot], done.at[slot]))
            copies[-1].start()
    for copy in copies:
        copy.wait()


def spread(x, rows, ys, cores, peers):
    tokens, width = x.shape
    part = (tokens, width // cores)
    return pl.pallas_call(
        functools.partial(spread_kernel, rows, ys, cores, peers),
        out_shape=jax.ShapeDtypeStruct((cores * peers, *part), x.dtype),
        in_specs=[pl.BlockSpec(memory_space=pltpu.VMEM)],
        out_specs=pl.BlockSpec(memory_space=pltpu.HBM),
        scratch_shapes=[
            pltpu.VMEM((cores, *part), x.dtype),
            pltpu.SemaphoreType.DMA((cores * peers,)),
        ],
        cost_estimate=pl.CostEstimate(
            flops=2 * tokens * width * width, bytes_accessed=10**6, transcendentals=0
        ),
        compiler_params=pltpu.CompilerParams(vmem_limit_bytes=VMEM_LIMIT),
        name="spread",
    )(x)


def stacked(block, at):
    block = block.astype(jnp.float32)
    lane = lax.broadcasted_iota(jnp.int32, (BLOCK, 2 * DH), 1)
    keep = (lane >= at) & (lane < at + DH)
    parts = []
    for head in range(block.shape[1] // DH):
        pair = block[:, (head // 2) * 2 * DH : (head // 2 + 1) * 2 * DH]
        if (head % 2) * DH != at:
            pair = pltpu.roll(pair, DH, 1)
        parts.append(jnp.where(keep, pair, 0.0))
    return jnp.concatenate(parts, axis=0)


def row_sums(terms, pieces):
    ones = jnp.ones((8, terms.shape[1]), jnp.bfloat16)
    total = None
    for _ in range(pieces):
        piece = terms.astype(jnp.bfloat16)
        terms = terms - piece.astype(jnp.float32)
        part = dot(ones, piece, NT)
        total = part if total is None else total + part
    return total[:1]


def terms(kv, low, high, lse, delta, keep=None):
    weights = jnp.exp(dot(kv, low, NT) - lse)
    if keep is not None:
        weights = jnp.where(keep, weights, 0.0)
    dscores = (weights * (dot(kv, high, NT) - delta)).astype(jnp.bfloat16)
    grad_kv = dot(dscores, low) + dot(weights.astype(jnp.bfloat16), high)
    return dot(dscores, kv, TN), grad_kv


def own_kernel(q_ref, go_ref, ao_ref, lse_ref, kv_ref, low_ref, high_ref, rows_ref, part_ref, own_ref):
    heads = q_ref.shape[1] // DH
    key_at = lax.broadcasted_iota(jnp.int32, (BLOCK, heads * BLOCK), 0)
    query_at = lax.broadcasted_iota(jnp.int32, (BLOCK, heads * BLOCK), 1) & (BLOCK - 1)
    for b in range(q_ref.shape[0] // BLOCK):
        rows = slice(b * BLOCK, (b + 1) * BLOCK)
        low = stacked(q_ref[rows] * DH ** (-0.5), 0)
        high = stacked(go_ref[rows], DH)
        delta = row_sums(high * stacked(ao_ref[rows], DH), 2)
        lse = jnp.concatenate([lse_ref[h : h + 1, rows] for h in range(heads)], axis=1)
        low = low.astype(jnp.bfloat16)
        high = high.astype(jnp.bfloat16)
        grad_q, grad_kv = terms(kv_ref[rows], low, high, lse, delta, key_at <= query_at)
        low_ref[b] = low
        high_ref[b] = high
        rows_ref[b, :1] = lse
        rows_ref[b, 1:] = delta
        part_ref[b] = grad_q
        own_ref[rows] = grad_kv


def attend_own(q, go, ao, lse, kv):
    tokens, width = q.shape
    blocks, rows = tokens // BLOCK, width * BLOCK // DH
    shape = (jax.ShapeDtypeStruct((blocks, rows, 2 * DH), jnp.bfloat16),) * 2
    shape += (jax.ShapeDtypeStruct((blocks, 2, rows), jnp.float32),)
    shape += (jax.ShapeDtypeStruct((blocks, rows, 2 * DH), jnp.float32),)
    shape += (jax.ShapeDtypeStruct(kv.shape, jnp.float32),)
    return call(own_kernel, 10**9, shape, q, go, ao, lse, kv)


def chosen_places(chosen_ref, distances, levels, blocks):
    me = lax.axis_index(KV)
    first = me * blocks
    start = jnp.minimum(first // LANES * LANES, chosen_ref.shape[1] - LANES * WINDOWS)
    columns = lax.broadcasted_iota(jnp.int32, (LEVELS * PER, LANES), 1)
    picked = [jnp.zeros((LEVELS * PER, LANES), jnp.int32)] * blocks
    for window in range(WINDOWS):
        tile = chosen_ref[:, pl.ds(pl.multiple_of(start + window * LANES, LANES), LANES)]
        for b in range(blocks):
            here = columns == first + b - start - window * LANES
            picked[b] = picked[b] + jnp.where(here, tile, 0)
    places = []
    for tile in picked:
        column = jnp.sum(tile.astype(jnp.float32), axis=1, keepdims=True).astype(jnp.int32)
        row = {}
        for level in levels:
            for n in range(PER):
                block = column[level * PER + n, 0]
                block = jnp.where(block >= 0, block - (me - distances[level]) * blocks, 0)
                row[level, n] = pl.ds(pl.multiple_of(block * BLOCK, BLOCK), BLOCK)
        places.append(row)
    return places


def far_terms(places, far_refs, low_ref, high_ref, rows_ref, sums, b):
    kv = jnp.concatenate([far_refs[level][at, :] for (level, _), at in places.items()], axis=0)
    grad_q, grad_kv = terms(kv, low_ref[b], high_ref[b], rows_ref[b, :1], rows_ref[b, 1:])
    for n, ((level, _), at) in enumerate(places.items()):
        sums[level][at, :] += grad_kv[n * BLOCK : (n + 1) * BLOCK]
    return grad_q


def far_kernel(distances, chosen_ref, low_ref, high_ref, rows_ref, part_ref, *refs):
    *step_refs, traded_ref, fetched_ref, passed_ref, out_ref = refs[:6]
    back_refs, (two_ref, four_ref) = refs[6 : 5 + LEVELS], refs[-2:]
    sums = dict(zip(range(1, LEVELS), refs[5 + LEVELS : -2]))
    at, quarter = lax.axis_index("z"), lax.axis_size("z") // 4
    in_second = jnp.logical_and(at >= quarter, at < 2 * quarter)
    is_late = lax.axis_index(KV) - distances[1] >= lax.axis_size(KV) // 2
    two_ref[...] = jnp.where(is_late, step_refs[1][...], step_refs[0][...])
    four_ref[...] = jnp.where(in_second, traded_ref[...], fetched_ref[...])
    far_refs = {1: two_ref, 2: four_ref, 3: passed_ref}
    for level in sums:
        sums[level][...] = jnp.zeros_like(sums[level])
    blocks = low_ref.shape[0]
    places = chosen_places(chosen_ref, distances, tuple(sums), blocks)
    for b in range(blocks):
        grad_q = far_terms(places[b], far_refs, low_ref, high_ref, rows_ref, sums, b)
        out_ref[b] = part_ref[b] + grad_q
    for level, back_ref in zip(sums, back_refs):
        back_ref[...] = sums[level][...].astype(back_ref.dtype)


def attend_far(distances, chosen, low, high, rows, part, far):
    kv = far[0]
    shape = (jax.ShapeDtypeStruct(part.shape, part.dtype),)
    shape += (jax.ShapeDtypeStruct(kv.shape, jnp.bfloat16),) * (LEVELS - 1)
    scratch = [pltpu.VMEM(kv.shape, jnp.float32)] * (LEVELS - 1) + [pltpu.VMEM(kv.shape, kv.dtype)] * 2
    kernel = functools.partial(far_kernel, distances)
    args = (chosen, low, high, rows, part, *far)
    return call(kernel, 2 * 10**9, shape, *args, scratch=scratch)


def near_kernel(distances, chosen_ref, low_ref, high_ref, rows_ref, part_ref, one_ref, gq_ref, back_ref, total):
    blocks, heads = low_ref.shape[0], low_ref.shape[1] // BLOCK
    lane = lax.broadcasted_iota(jnp.int32, (BLOCK, 2 * DH), 1)
    total[...] = jnp.zeros_like(total)
    places = chosen_places(chosen_ref, distances, (0,), blocks)
    for b in range(blocks):
        rows = slice(b * BLOCK, (b + 1) * BLOCK)
        grad_q = far_terms(places[b], {0: one_ref}, low_ref, high_ref, rows_ref, {0: total}, b)
        grad_q = (part_ref[b] + grad_q) * DH ** (-0.5)
        for pair in range(heads // 2):
            first = grad_q[2 * pair * BLOCK : (2 * pair + 1) * BLOCK]
            second = grad_q[(2 * pair + 1) * BLOCK : (2 * pair + 2) * BLOCK]
            gq_ref[rows, pair * 2 * DH : (pair + 1) * 2 * DH] = jnp.where(
                lane < DH, first, pltpu.roll(second, DH, 1)
            ).astype(gq_ref.dtype)
    back_ref[...] = total[...].astype(back_ref.dtype)


def attend_near(distances, chosen, low, high, rows, part, near):
    tokens, width = low.shape[0] * BLOCK, low.shape[1] * DH // BLOCK
    shape = (
        jax.ShapeDtypeStruct((tokens, width), jnp.bfloat16),
        jax.ShapeDtypeStruct(near.shape, jnp.bfloat16),
    )
    kernel = functools.partial(near_kernel, distances)
    args = (chosen, low, high, rows, part, near)
    return call(kernel, 10**9, shape, *args, scratch=[pltpu.VMEM(near.shape, jnp.float32)])


def weight_kernel(mine_ref, other_ref, x_ref, out_ref, held, done):
    core = lax.axis_index("c")
    peers = x_ref.shape[0] // 2
    ys = out_ref.shape[0]
    step = x_ref.shape[2] // ys
    grads = jnp.concatenate([mine_ref[...], other_ref[...]], axis=0)
    copies = []
    for half in range(2):
        mine = range(half * ys // 2, (half + 1) * ys // 2)
        lanes = slice(mine[0] * step, (mine[-1] + 1) * step)
        for peer in range(peers):
            slots = [X_ORDER.index(c * peers + peer) for c in range(2)]
            first, second = jnp.where(core == 0, *slots), jnp.where(core == 0, *slots[::-1])
            x = jnp.concatenate([x_ref[first, :, lanes], x_ref[second, :, lanes]], axis=0)
            part = dot(x, grads, TN).astype(held.dtype)
            for n, y in enumerate(mine):
                held[y, peer * step : (peer + 1) * step] = part[n * step : (n + 1) * step]
        for y in mine:
            slot = jnp.where(core == 0, *(order.index(y) for order in Y_ORDERS))
            copies.append(pltpu.make_async_copy(held.at[y], out_ref.at[slot], done.at[y]))
            copies[-1].start()
    for copy in copies:
        copy.wait()


def weight(mine, other, x, ys):
    peers, tokens, part = x.shape[0] // 2, x.shape[1], x.shape[2]
    shape = (ys, peers * part // ys, mine.shape[1])
    vmem = pl.BlockSpec(memory_space=pltpu.VMEM)
    return pl.pallas_call(
        weight_kernel,
        out_shape=jax.ShapeDtypeStruct(shape, jnp.bfloat16),
        in_specs=[vmem] * 3,
        out_specs=pl.BlockSpec(memory_space=pltpu.HBM),
        scratch_shapes=[pltpu.VMEM(shape, jnp.bfloat16), pltpu.SemaphoreType.DMA((ys,))],
        cost_estimate=pl.CostEstimate(
            flops=4 * tokens * peers * part * mine.shape[1], bytes_accessed=10**6, transcendentals=0
        ),
        compiler_params=pltpu.CompilerParams(vmem_limit_bytes=VMEM_LIMIT),
        name="weight",
    )(mine, other, x)


def sum_kernel(order, tiles_ref, out_ref):
    total = tiles_ref[0].astype(jnp.float32)
    for n in range(1, tiles_ref.shape[0]):
        total = total + tiles_ref[n].astype(jnp.float32)
    total = total.astype(out_ref.dtype)
    if order is None:
        out_ref[...] = total
    else:
        for slot, place in enumerate(order):
            out_ref[slot] = total[place]


def summed(tiles, dtype, order=None):
    shape = jax.ShapeDtypeStruct(tiles.shape[1:], dtype)
    return call(functools.partial(sum_kernel, order), tiles.size, shape, tiles)


def collect_kernel(grads_ref, own_ref, *refs):
    *parts, gq_ref, gk_ref, gv_ref = refs
    total = own_ref[...]
    for ref in parts:
        total = total + ref[...].astype(jnp.float32)
    total = turned(total)
    width = total.shape[0] // 2
    gq_ref[...] = grads_ref[...]
    gk_ref[...] = total[:width].astype(jnp.bfloat16)
    gv_ref[...] = total[width:].astype(jnp.bfloat16)


def collect(grads, own, back):
    shape = jax.ShapeDtypeStruct((own.shape[1] // 2, own.shape[0]), jnp.bfloat16)
    shapes = (jax.ShapeDtypeStruct(grads.shape, grads.dtype), shape, shape)
    return call(collect_kernel, 10**6, shapes, grads, own, *back)


def shards(layer_input, queries, keys, values, attn_out, grad_out, log_sum, chosen):
    axis_size = lax.axis_size(KV)
    ys, cores, peers = lax.axis_size("y"), lax.axis_size("c"), lax.axis_size("x")
    out_rows = layer_input.shape[1] * peers // axis_size
    distances = [1, axis_size // 8, axis_size // 4, axis_size // 2]
    key_pair = pack(keys.T, values.T)
    near = shifted(key_pair, KV, distances[0])
    halves = [range(axis_size // 2), range(axis_size // 2, axis_size)]
    steps = []
    for senders in halves:
        steps.append(shifted(key_pair, KV, distances[1], senders))
    quarter = lax.axis_size("z") // 4
    quarters = [range(n * quarter, (n + 1) * quarter) for n in range(4)]
    traded = between(key_pair, quarters, ((0, 1), (1, 0)))
    passed = between(traded, quarters, ((1, 2), (0, 3)))
    fetched = between(key_pair, quarters, ((1, 2), (2, 3)))
    far = [*steps, traded, fetched, passed]
    sent = spread(layer_input, out_rows, ys, cores, peers)
    whole_input = exchanged(sent, ("c", "x"), [list(X_ORDER)])
    *staged, part, grad_own = attend_own(queries, grad_out, attn_out, log_sum.T, key_pair)
    part, *back = attend_far(distances, chosen.T, *staged, part, far)
    grads, back_near = attend_near(distances, chosen.T, *staged, part, near)
    back = [back_near, *back]
    route = [(i, cores - 1 - i) for i in range(cores)]
    other = lax.ppermute(grads, "c", route)
    parts = weight(grads, other, whole_input, ys)
    groups = [[y * cores + c for y in order] for c, order in enumerate(Y_ORDERS)]
    over_y = exchanged(parts, ("y", "c"), groups)
    returned = []
    for level, distance in enumerate(distances[:-1]):
        for receivers in halves:
            block = shifted(back[level], KV, -distance, receivers=receivers)
            returned.append(block)
    returned.append(shifted(back[-1], KV, -distances[-1]))
    over_y = summed(over_y.reshape(ys, -1, out_rows, over_y.shape[2]), jnp.bfloat16, Z_ORDER)
    over_z = exchanged(over_y, "z", [list(Z_ORDER)])
    grad_queries, grad_keys, grad_values = collect(grads, grad_own, returned)
    grad_weight = summed(over_z, jnp.float32)
    return (grad_queries, grad_keys.T, grad_values.T, grad_weight)


def solution(mesh):
    ys, cores = SIDES
    shape = (mesh.shape["kv"] // (ys * cores), ys, cores, mesh.shape["tp"])
    torus = Mesh(mesh.devices.reshape(shape), (*KV, "x"))
    return jax.shard_map(
        shards,
        mesh=torus,
        in_specs=(P(KV, "x"),) * 7 + (P(),),
        out_specs=(P(KV, "x"),) * 4,
        check_vma=False,
    )
```

```python
import functools

import jax
import jax.numpy as jnp
from jax import lax
from jax.experimental import pallas as pl
from jax.experimental.pallas import tpu as pltpu
from jax.sharding import Mesh
from jax.sharding import PartitionSpec as P

DH = 64
BLOCK = 64
PER = 2
LEVELS = 4
SIDES = (8, 2)
KV = ("z", "y", "c")
NT = (((1,), (1,)), ((), ()))
TN = (((0,), (0,)), ((), ()))
Y_ORDERS = ((3, 2, 1, 0, 7, 6, 5, 4), (5, 6, 7, 0, 1, 2, 3, 4))
Z_ORDER = (8, 9, 10, 11, 12, 13, 14, 15, 0, 1, 2, 3, 4, 5, 6, 7)
X_ORDER = (5, 4, 6, 7, 1, 0, 2, 3)
LANES = 128
WINDOWS = 2
VMEM_LIMIT = 16 * 2**20


def shifted(block, axis, distance, senders=None, receivers=None):
    devices = range(lax.axis_size(axis))
    senders, receivers = senders or devices, receivers or devices
    route = [(i, i + distance) for i in senders if i + distance in receivers]
    return lax.ppermute(block, axis, route)


def between(block, quarters, pairs):
    route = [p for a, b in pairs for p in zip(quarters[a], quarters[b])]
    return lax.ppermute(block, "z", route)


def exchanged(tiles, axis, groups=None):
    return lax.all_to_all(
        tiles, axis, split_axis=0, concat_axis=0, tiled=True, axis_index_groups=groups
    )


def dot(a, b, dims=(((1,), (0,)), ((), ()))):
    return lax.dot_general(a, b, dims, preferred_element_type=jnp.float32)


def call(kernel, flops, out_shape, *args, smem=0, scratch=()):
    vmem = pl.BlockSpec(memory_space=pltpu.VMEM)
    many = isinstance(out_shape, tuple)
    size = sum(a.size * a.dtype.itemsize for a in args)
    return pl.pallas_call(
        kernel,
        out_shape=out_shape,
        in_specs=[pl.BlockSpec(memory_space=pltpu.SMEM)] * smem + [vmem] * (len(args) - smem),
        out_specs=(vmem,) * len(out_shape) if many else vmem,
        scratch_shapes=scratch,
        cost_estimate=pl.CostEstimate(flops=flops, bytes_accessed=size, transcendentals=0),
        compiler_params=pltpu.CompilerParams(vmem_limit_bytes=VMEM_LIMIT),
    )(*args)


def turned(x):
    return jnp.transpose(x.astype(jnp.float32))


def pack_kernel(kv_ref, out_ref):
    out_ref[...] = turned(kv_ref[...]).astype(out_ref.dtype)


def pack(k, v):
    kv = jnp.concatenate([k, v], axis=0)
    shape = jax.ShapeDtypeStruct(kv.shape[::-1], kv.dtype)
    return call(pack_kernel, 10**10, shape, kv)


def spread_kernel(rows, ys, cores, peers, x_ref, out_ref, held, done):
    width = x_ref.shape[1]
    source = lax.broadcasted_iota(jnp.int32, (width, 1), 0)
    inner, left = source & (rows - 1), source // rows
    core, left = left & (cores - 1), left // cores
    y, z = left & (ys - 1), left // ys
    zs = width // (rows * cores * ys)
    place = ((core * ys + y) * zs + z) * rows + inner
    part = width // cores
    target = lax.broadcasted_iota(jnp.int32, (width, part), 1)
    copies = []
    for core in range(cores):
        move = jnp.where(place == target + core * part, 1.0, 0.0).astype(jnp.bfloat16)
        held[core] = dot(x_ref[...], move).astype(jnp.bfloat16)
        for peer in range(peers):
            slot = X_ORDER.index(core * peers + peer)
            copies.append(pltpu.make_async_copy(held.at[core], out_ref.at[slot], done.at[slot]))
            copies[-1].start()
    for copy in copies:
        copy.wait()


def spread(x, rows, ys, cores, peers):
    tokens, width = x.shape
    part = (tokens, width // cores)
    return pl.pallas_call(
        functools.partial(spread_kernel, rows, ys, cores, peers),
        out_shape=jax.ShapeDtypeStruct((cores * peers, *part), x.dtype),
        in_specs=[pl.BlockSpec(memory_space=pltpu.VMEM)],
        out_specs=pl.BlockSpec(memory_space=pltpu.HBM),
        scratch_shapes=[
            pltpu.VMEM((cores, *part), x.dtype),
            pltpu.SemaphoreType.DMA((cores * peers,)),
        ],
        cost_estimate=pl.CostEstimate(
            flops=2 * tokens * width * width, bytes_accessed=10**6, transcendentals=0
        ),
        compiler_params=pltpu.CompilerParams(vmem_limit_bytes=VMEM_LIMIT),
        name="spread",
    )(x)


def stacked(block, at):
    block = block.astype(jnp.float32)
    lane = lax.broadcasted_iota(jnp.int32, (BLOCK, 2 * DH), 1)
    keep = (lane >= at) & (lane < at + DH)
    parts = []
    for head in range(block.shape[1] // DH):
        pair = block[:, (head // 2) * 2 * DH : (head // 2 + 1) * 2 * DH]
        if (head % 2) * DH != at:
            pair = pltpu.roll(pair, DH, 1)
        parts.append(jnp.where(keep, pair, 0.0))
    return jnp.concatenate(parts, axis=0)


def row_sums(terms, pieces):
    ones = jnp.ones((8, terms.shape[1]), jnp.bfloat16)
    total = None
    for _ in range(pieces):
        piece = terms.astype(jnp.bfloat16)
        terms = terms - piece.astype(jnp.float32)
        part = dot(ones, piece, NT)
        total = part if total is None else total + part
    return total[:1]


def terms(kv, low, high, lse, delta, keep=None):
    weights = jnp.exp(dot(kv, low, NT) - lse)
    if keep is not None:
        weights = jnp.where(keep, weights, 0.0)
    dscores = (weights * (dot(kv, high, NT) - delta)).astype(jnp.bfloat16)
    grad_kv = dot(dscores, low) + dot(weights.astype(jnp.bfloat16), high)
    return dot(dscores, kv, TN), grad_kv


def own_kernel(q_ref, go_ref, ao_ref, lse_ref, kv_ref, low_ref, high_ref, rows_ref, part_ref, own_ref):
    heads = q_ref.shape[1] // DH
    key_at = lax.broadcasted_iota(jnp.int32, (BLOCK, heads * BLOCK), 0)
    query_at = lax.broadcasted_iota(jnp.int32, (BLOCK, heads * BLOCK), 1) & (BLOCK - 1)
    for b in range(q_ref.shape[0] // BLOCK):
        rows = slice(b * BLOCK, (b + 1) * BLOCK)
        low = stacked(q_ref[rows] * DH ** (-0.5), 0)
        high = stacked(go_ref[rows], DH)
        delta = row_sums(high * stacked(ao_ref[rows], DH), 2)
        lse = jnp.concatenate([lse_ref[h : h + 1, rows] for h in range(heads)], axis=1)
        low = low.astype(jnp.bfloat16)
        high = high.astype(jnp.bfloat16)
        grad_q, grad_kv = terms(kv_ref[rows], low, high, lse, delta, key_at <= query_at)
        low_ref[b] = low
        high_ref[b] = high
        rows_ref[b, :1] = lse
        rows_ref[b, 1:] = delta
        part_ref[b] = grad_q
        own_ref[rows] = grad_kv


def attend_own(q, go, ao, lse, kv):
    tokens, width = q.shape
    blocks, rows = tokens // BLOCK, width * BLOCK // DH
    shape = (jax.ShapeDtypeStruct((blocks, rows, 2 * DH), jnp.bfloat16),) * 2
    shape += (jax.ShapeDtypeStruct((blocks, 2, rows), jnp.float32),)
    shape += (jax.ShapeDtypeStruct((blocks, rows, 2 * DH), jnp.float32),)
    shape += (jax.ShapeDtypeStruct(kv.shape, jnp.float32),)
    return call(own_kernel, 10**9, shape, q, go, ao, lse, kv)


def chosen_places(chosen_ref, distances, levels, blocks):
    me = lax.axis_index(KV)
    first = me * blocks
    start = jnp.minimum(first // LANES * LANES, chosen_ref.shape[1] - LANES * WINDOWS)
    columns = lax.broadcasted_iota(jnp.int32, (LEVELS * PER, LANES), 1)
    picked = [jnp.zeros((LEVELS * PER, LANES), jnp.int32)] * blocks
    for window in range(WINDOWS):
        tile = chosen_ref[:, pl.ds(pl.multiple_of(start + window * LANES, LANES), LANES)]
        for b in range(blocks):
            here = columns == first + b - start - window * LANES
            picked[b] = picked[b] + jnp.where(here, tile, 0)
    places = []
    for tile in picked:
        column = jnp.sum(tile.astype(jnp.float32), axis=1, keepdims=True).astype(jnp.int32)
        row = {}
        for level in levels:
            for n in range(PER):
                block = column[level * PER + n, 0]
                block = jnp.where(block >= 0, block - (me - distances[level]) * blocks, 0)
                row[level, n] = pl.ds(pl.multiple_of(block * BLOCK, BLOCK), BLOCK)
        places.append(row)
    return places


def far_terms(places, far_refs, low_ref, high_ref, rows_ref, sums, b):
    kv = jnp.concatenate([far_refs[level][at, :] for (level, _), at in places.items()], axis=0)
    grad_q, grad_kv = terms(kv, low_ref[b], high_ref[b], rows_ref[b, :1], rows_ref[b, 1:])
    for n, ((level, _), at) in enumerate(places.items()):
        sums[level][at, :] += grad_kv[n * BLOCK : (n + 1) * BLOCK]
    return grad_q


def comes_late(distances):
    return lax.axis_index(KV) - distances[1] >= lax.axis_size(KV) // 2


def far_kernel(distances, chosen_ref, low_ref, high_ref, rows_ref, part_ref, *refs):
    early_ref, traded_ref, fetched_ref, passed_ref, out_ref, *back_refs = refs[: 4 + LEVELS]
    four_ref, *totals = refs[4 + LEVELS :]
    sums = dict(zip(range(1, LEVELS), totals))
    at, quarter = lax.axis_index("z"), lax.axis_size("z") // 4
    in_second = jnp.logical_and(at >= quarter, at < 2 * quarter)
    four_ref[...] = jnp.where(in_second, traded_ref[...], fetched_ref[...])
    far_refs = {1: early_ref, 2: four_ref, 3: passed_ref}
    for total in totals:
        total[...] = jnp.zeros_like(total)
    blocks = low_ref.shape[0]
    is_late = comes_late(distances)

    def attend(levels):
        places = chosen_places(chosen_ref, distances, levels, blocks)
        for b in range(blocks):
            grad_q = far_terms(places[b], far_refs, low_ref, high_ref, rows_ref, sums, b)
            out_ref[b] = part_ref[b] + grad_q

    pl.when(is_late)(lambda: attend((2, 3)))
    pl.when(jnp.logical_not(is_late))(lambda: attend((1, 2, 3)))
    for total, back_ref in zip(totals, back_refs):
        back_ref[...] = total[...].astype(back_ref.dtype)


def attend_far(distances, chosen, low, high, rows, part, far):
    kv = far[0]
    shape = (jax.ShapeDtypeStruct(part.shape, part.dtype),)
    shape += (jax.ShapeDtypeStruct(kv.shape, jnp.bfloat16),) * (LEVELS - 1)
    scratch = [pltpu.VMEM(kv.shape, kv.dtype)] + [pltpu.VMEM(kv.shape, jnp.float32)] * (LEVELS - 1)
    kernel = functools.partial(far_kernel, distances)
    args = (chosen, low, high, rows, part, *far)
    return call(kernel, 2 * 10**9, shape, *args, scratch=scratch)


def near_kernel(distances, chosen_ref, low_ref, high_ref, rows_ref, part_ref, *refs):
    one_ref, late_ref, found_ref, gq_ref, one_back_ref, two_back_ref, *totals = refs
    blocks, heads = low_ref.shape[0], low_ref.shape[1] // BLOCK
    lane = lax.broadcasted_iota(jnp.int32, (BLOCK, 2 * DH), 1)
    sums = dict(enumerate(totals))
    is_late = comes_late(distances)
    for total in totals:
        total[...] = jnp.zeros_like(total)

    def attend(levels):
        places = chosen_places(chosen_ref, distances, levels, blocks)
        for b in range(blocks):
            rows = slice(b * BLOCK, (b + 1) * BLOCK)
            near_refs = {0: one_ref, 1: late_ref}
            grad_q = far_terms(places[b], near_refs, low_ref, high_ref, rows_ref, sums, b)
            grad_q = (part_ref[b] + grad_q) * DH ** (-0.5)
            for pair in range(heads // 2):
                first = grad_q[2 * pair * BLOCK : (2 * pair + 1) * BLOCK]
                second = grad_q[(2 * pair + 1) * BLOCK : (2 * pair + 2) * BLOCK]
                gq_ref[rows, pair * 2 * DH : (pair + 1) * 2 * DH] = jnp.where(
                    lane < DH, first, pltpu.roll(second, DH, 1)
                ).astype(gq_ref.dtype)

    pl.when(is_late)(lambda: attend((0, 1)))
    pl.when(jnp.logical_not(is_late))(lambda: attend((0,)))
    one_back_ref[...] = totals[0][...].astype(one_back_ref.dtype)
    two_back = totals[1][...].astype(two_back_ref.dtype)
    two_back_ref[...] = jnp.where(is_late, two_back, found_ref[...])


def attend_near(distances, chosen, low, high, rows, part, near, late, found):
    tokens, width = low.shape[0] * BLOCK, low.shape[1] * DH // BLOCK
    shape = (jax.ShapeDtypeStruct((tokens, width), jnp.bfloat16),)
    shape += (jax.ShapeDtypeStruct(near.shape, jnp.bfloat16),) * 2
    kernel = functools.partial(near_kernel, distances)
    args = (chosen, low, high, rows, part, near, late, found)
    scratch = [pltpu.VMEM(near.shape, jnp.float32)] * 2
    return call(kernel, 10**9, shape, *args, scratch=scratch)


def weight_kernel(mine_ref, other_ref, x_ref, out_ref, held, done):
    core = lax.axis_index("c")
    peers = x_ref.shape[0] // 2
    ys = out_ref.shape[0]
    step = x_ref.shape[2] // ys
    grads = jnp.concatenate([mine_ref[...], other_ref[...]], axis=0)
    copies = []
    for half in range(2):
        mine = range(half * ys // 2, (half + 1) * ys // 2)
        lanes = slice(mine[0] * step, (mine[-1] + 1) * step)
        for peer in range(peers):
            slots = [X_ORDER.index(c * peers + peer) for c in range(2)]
            first, second = jnp.where(core == 0, *slots), jnp.where(core == 0, *slots[::-1])
            x = jnp.concatenate([x_ref[first, :, lanes], x_ref[second, :, lanes]], axis=0)
            part = dot(x, grads, TN).astype(held.dtype)
            for n, y in enumerate(mine):
                held[y, peer * step : (peer + 1) * step] = part[n * step : (n + 1) * step]
        for y in mine:
            slot = jnp.where(core == 0, *(order.index(y) for order in Y_ORDERS))
            copies.append(pltpu.make_async_copy(held.at[y], out_ref.at[slot], done.at[y]))
            copies[-1].start()
    for copy in copies:
        copy.wait()


def weight(mine, other, x, ys):
    peers, tokens, part = x.shape[0] // 2, x.shape[1], x.shape[2]
    shape = (ys, peers * part // ys, mine.shape[1])
    vmem = pl.BlockSpec(memory_space=pltpu.VMEM)
    return pl.pallas_call(
        weight_kernel,
        out_shape=jax.ShapeDtypeStruct(shape, jnp.bfloat16),
        in_specs=[vmem] * 3,
        out_specs=pl.BlockSpec(memory_space=pltpu.HBM),
        scratch_shapes=[pltpu.VMEM(shape, jnp.bfloat16), pltpu.SemaphoreType.DMA((ys,))],
        cost_estimate=pl.CostEstimate(
            flops=4 * tokens * peers * part * mine.shape[1], bytes_accessed=10**6, transcendentals=0
        ),
        compiler_params=pltpu.CompilerParams(vmem_limit_bytes=VMEM_LIMIT),
        name="weight",
    )(mine, other, x)


def sum_kernel(order, tiles_ref, out_ref):
    total = tiles_ref[0].astype(jnp.float32)
    for n in range(1, tiles_ref.shape[0]):
        total = total + tiles_ref[n].astype(jnp.float32)
    total = total.astype(out_ref.dtype)
    if order is None:
        out_ref[...] = total
    else:
        for slot, place in enumerate(order):
            out_ref[slot] = total[place]


def summed(tiles, dtype, order=None):
    shape = jax.ShapeDtypeStruct(tiles.shape[1:], dtype)
    return call(functools.partial(sum_kernel, order), tiles.size, shape, tiles)


def collect_kernel(grads_ref, own_ref, *refs):
    *parts, gq_ref, gk_ref, gv_ref = refs
    total = own_ref[...]
    for ref in parts:
        total = total + ref[...].astype(jnp.float32)
    total = turned(total)
    width = total.shape[0] // 2
    gq_ref[...] = grads_ref[...]
    gk_ref[...] = total[:width].astype(jnp.bfloat16)
    gv_ref[...] = total[width:].astype(jnp.bfloat16)


def collect(grads, own, back):
    shape = jax.ShapeDtypeStruct((own.shape[1] // 2, own.shape[0]), jnp.bfloat16)
    shapes = (jax.ShapeDtypeStruct(grads.shape, grads.dtype), shape, shape)
    return call(collect_kernel, 10**6, shapes, grads, own, *back)


def shards(layer_input, queries, keys, values, attn_out, grad_out, log_sum, chosen):
    axis_size = lax.axis_size(KV)
    ys, cores, peers = lax.axis_size("y"), lax.axis_size("c"), lax.axis_size("x")
    out_rows = layer_input.shape[1] * peers // axis_size
    distances = [1, axis_size // 8, axis_size // 4, axis_size // 2]
    key_pair = pack(keys.T, values.T)
    near = shifted(key_pair, KV, distances[0])
    halves = [range(axis_size // 2), range(axis_size // 2, axis_size)]
    steps = []
    for senders in halves:
        steps.append(shifted(key_pair, KV, distances[1], senders))
    quarter = lax.axis_size("z") // 4
    quarters = [range(n * quarter, (n + 1) * quarter) for n in range(4)]
    traded = between(key_pair, quarters, ((0, 1), (1, 0)))
    passed = between(traded, quarters, ((1, 2), (0, 3)))
    fetched = between(key_pair, quarters, ((1, 2), (2, 3)))
    far = [steps[0], traded, fetched, passed]
    sent = spread(layer_input, out_rows, ys, cores, peers)
    whole_input = exchanged(sent, ("c", "x"), [list(X_ORDER)])
    *staged, part, grad_own = attend_own(queries, grad_out, attn_out, log_sum.T, key_pair)
    part, found, *back_far = attend_far(distances, chosen.T, *staged, part, far)
    near = (near, steps[1], found)
    grads, *back = attend_near(distances, chosen.T, *staged, part, *near)
    back += back_far
    route = [(i, cores - 1 - i) for i in range(cores)]
    other = lax.ppermute(grads, "c", route)
    parts = weight(grads, other, whole_input, ys)
    groups = [[y * cores + c for y in order] for c, order in enumerate(Y_ORDERS)]
    over_y = exchanged(parts, ("y", "c"), groups)
    returned = []
    for level, distance in enumerate(distances[:-1]):
        for receivers in halves:
            block = shifted(back[level], KV, -distance, receivers=receivers)
            returned.append(block)
    returned.append(shifted(back[-1], KV, -distances[-1]))
    over_y = summed(over_y.reshape(ys, -1, out_rows, over_y.shape[2]), jnp.bfloat16, Z_ORDER)
    over_z = exchanged(over_y, "z", [list(Z_ORDER)])
    grad_queries, grad_keys, grad_values = collect(grads, grad_own, returned)
    grad_weight = summed(over_z, jnp.float32)
    return (grad_queries, grad_keys.T, grad_values.T, grad_weight)


def solution(mesh):
    ys, cores = SIDES
    shape = (mesh.shape["kv"] // (ys * cores), ys, cores, mesh.shape["tp"])
    torus = Mesh(mesh.devices.reshape(shape), (*KV, "x"))
    return jax.shard_map(
        shards,
        mesh=torus,
        in_specs=(P(KV, "x"),) * 7 + (P(),),
        out_specs=(P(KV, "x"),) * 4,
        check_vma=False,
    )
```

```python
import functools

import jax
import jax.numpy as jnp
from jax import lax
from jax.experimental import pallas as pl
from jax.experimental.pallas import tpu as pltpu
from jax.sharding import Mesh
from jax.sharding import PartitionSpec as P

DH = 64
BLOCK = 64
PER = 2
LEVELS = 4
SIDES = (8, 2)
KV = ("z", "y", "c")
NT = (((1,), (1,)), ((), ()))
TN = (((0,), (0,)), ((), ()))
Y_ORDERS = ((3, 2, 1, 0, 7, 6, 5, 4), (5, 6, 7, 0, 1, 2, 3, 4))
Z_ORDER = (8, 9, 10, 11, 12, 13, 14, 15, 0, 1, 2, 3, 4, 5, 6, 7)
X_ORDER = (5, 1, 6, 2, 7, 3, 4, 0)
LANES = 128
WINDOWS = 2
VMEM_LIMIT = 16 * 2**20


def shifted(block, axis, distance, senders=None, receivers=None):
    devices = range(lax.axis_size(axis))
    senders, receivers = senders or devices, receivers or devices
    route = [(i, i + distance) for i in senders if i + distance in receivers]
    return lax.ppermute(block, axis, route)


def between(block, quarters, pairs):
    route = [p for a, b in pairs for p in zip(quarters[a], quarters[b])]
    return lax.ppermute(block, "z", route)


def exchanged(tiles, axis, groups=None):
    return lax.all_to_all(
        tiles, axis, split_axis=0, concat_axis=0, tiled=True, axis_index_groups=groups
    )


def dot(a, b, dims=(((1,), (0,)), ((), ()))):
    return lax.dot_general(a, b, dims, preferred_element_type=jnp.float32)


def call(kernel, flops, out_shape, *args, smem=0, scratch=()):
    vmem = pl.BlockSpec(memory_space=pltpu.VMEM)
    many = isinstance(out_shape, tuple)
    size = sum(a.size * a.dtype.itemsize for a in args)
    return pl.pallas_call(
        kernel,
        out_shape=out_shape,
        in_specs=[pl.BlockSpec(memory_space=pltpu.SMEM)] * smem + [vmem] * (len(args) - smem),
        out_specs=(vmem,) * len(out_shape) if many else vmem,
        scratch_shapes=scratch,
        cost_estimate=pl.CostEstimate(flops=flops, bytes_accessed=size, transcendentals=0),
        compiler_params=pltpu.CompilerParams(vmem_limit_bytes=VMEM_LIMIT),
    )(*args)


def turned(x):
    return jnp.transpose(x.astype(jnp.float32))


def pack_kernel(kv_ref, out_ref):
    out_ref[...] = turned(kv_ref[...]).astype(out_ref.dtype)


def pack(k, v):
    kv = jnp.concatenate([k, v], axis=0)
    shape = jax.ShapeDtypeStruct(kv.shape[::-1], kv.dtype)
    return call(pack_kernel, 10**10, shape, kv)


def spread_kernel(rows, ys, cores, peers, x_ref, out_ref, held, done):
    width = x_ref.shape[1]
    source = lax.broadcasted_iota(jnp.int32, (width, 1), 0)
    inner, left = source & (rows - 1), source // rows
    core, left = left & (cores - 1), left // cores
    y, z = left & (ys - 1), left // ys
    zs = width // (rows * cores * ys)
    place = ((core * ys + y) * zs + z) * rows + inner
    part = width // cores
    target = lax.broadcasted_iota(jnp.int32, (width, part), 1)
    copies = []
    for core in range(cores):
        move = jnp.where(place == target + core * part, 1.0, 0.0).astype(jnp.bfloat16)
        held[core] = dot(x_ref[...], move).astype(jnp.bfloat16)
        for peer in range(peers):
            slot = X_ORDER.index(core * peers + peer)
            copies.append(pltpu.make_async_copy(held.at[core], out_ref.at[slot], done.at[slot]))
            copies[-1].start()
    for copy in copies:
        copy.wait()


def spread(x, rows, ys, cores, peers):
    tokens, width = x.shape
    part = (tokens, width // cores)
    return pl.pallas_call(
        functools.partial(spread_kernel, rows, ys, cores, peers),
        out_shape=jax.ShapeDtypeStruct((cores * peers, *part), x.dtype),
        in_specs=[pl.BlockSpec(memory_space=pltpu.VMEM)],
        out_specs=pl.BlockSpec(memory_space=pltpu.HBM),
        scratch_shapes=[
            pltpu.VMEM((cores, *part), x.dtype),
            pltpu.SemaphoreType.DMA((cores * peers,)),
        ],
        cost_estimate=pl.CostEstimate(
            flops=2 * tokens * width * width, bytes_accessed=10**6, transcendentals=0
        ),
        compiler_params=pltpu.CompilerParams(vmem_limit_bytes=VMEM_LIMIT),
        name="spread",
    )(x)


def stacked(block, at):
    block = block.astype(jnp.float32)
    lane = lax.broadcasted_iota(jnp.int32, (BLOCK, 2 * DH), 1)
    keep = (lane >= at) & (lane < at + DH)
    parts = []
    for head in range(block.shape[1] // DH):
        pair = block[:, (head // 2) * 2 * DH : (head // 2 + 1) * 2 * DH]
        if (head % 2) * DH != at:
            pair = pltpu.roll(pair, DH, 1)
        parts.append(jnp.where(keep, pair, 0.0))
    return jnp.concatenate(parts, axis=0)


def row_sums(terms, pieces):
    ones = jnp.ones((8, terms.shape[1]), jnp.bfloat16)
    total = None
    for _ in range(pieces):
        piece = terms.astype(jnp.bfloat16)
        terms = terms - piece.astype(jnp.float32)
        part = dot(ones, piece, NT)
        total = part if total is None else total + part
    return total[:1]


def terms(kv, low, high, lse, delta, keep=None):
    weights = jnp.exp(dot(kv, low, NT) - lse)
    if keep is not None:
        weights = jnp.where(keep, weights, 0.0)
    dscores = (weights * (dot(kv, high, NT) - delta)).astype(jnp.bfloat16)
    grad_kv = dot(dscores, low) + dot(weights.astype(jnp.bfloat16), high)
    return dot(dscores, kv, TN), grad_kv


def own_kernel(q_ref, go_ref, ao_ref, lse_ref, kv_ref, low_ref, high_ref, rows_ref, part_ref, own_ref):
    heads = q_ref.shape[1] // DH
    key_at = lax.broadcasted_iota(jnp.int32, (BLOCK, heads * BLOCK), 0)
    query_at = lax.broadcasted_iota(jnp.int32, (BLOCK, heads * BLOCK), 1) & (BLOCK - 1)
    for b in range(q_ref.shape[0] // BLOCK):
        rows = slice(b * BLOCK, (b + 1) * BLOCK)
        low = stacked(q_ref[rows] * DH ** (-0.5), 0)
        high = stacked(go_ref[rows], DH)
        delta = row_sums(high * stacked(ao_ref[rows], DH), 2)
        lse = jnp.concatenate([lse_ref[h : h + 1, rows] for h in range(heads)], axis=1)
        low = low.astype(jnp.bfloat16)
        high = high.astype(jnp.bfloat16)
        grad_q, grad_kv = terms(kv_ref[rows], low, high, lse, delta, key_at <= query_at)
        low_ref[b] = low
        high_ref[b] = high
        rows_ref[b, :1] = lse
        rows_ref[b, 1:] = delta
        part_ref[b] = grad_q
        own_ref[rows] = grad_kv


def attend_own(q, go, ao, lse, kv):
    tokens, width = q.shape
    blocks, rows = tokens // BLOCK, width * BLOCK // DH
    shape = (jax.ShapeDtypeStruct((blocks, rows, 2 * DH), jnp.bfloat16),) * 2
    shape += (jax.ShapeDtypeStruct((blocks, 2, rows), jnp.float32),)
    shape += (jax.ShapeDtypeStruct((blocks, rows, 2 * DH), jnp.float32),)
    shape += (jax.ShapeDtypeStruct(kv.shape, jnp.float32),)
    return call(own_kernel, 10**9, shape, q, go, ao, lse, kv)


def chosen_places(chosen_ref, distances, levels, blocks):
    me = lax.axis_index(KV)
    first = me * blocks
    start = jnp.minimum(first // LANES * LANES, chosen_ref.shape[1] - LANES * WINDOWS)
    columns = lax.broadcasted_iota(jnp.int32, (LEVELS * PER, LANES), 1)
    picked = [jnp.zeros((LEVELS * PER, LANES), jnp.int32)] * blocks
    for window in range(WINDOWS):
        tile = chosen_ref[:, pl.ds(pl.multiple_of(start + window * LANES, LANES), LANES)]
        for b in range(blocks):
            here = columns == first + b - start - window * LANES
            picked[b] = picked[b] + jnp.where(here, tile, 0)
    places = []
    for tile in picked:
        column = jnp.sum(tile.astype(jnp.float32), axis=1, keepdims=True).astype(jnp.int32)
        row = {}
        for level in levels:
            for n in range(PER):
                block = column[level * PER + n, 0]
                block = jnp.where(block >= 0, block - (me - distances[level]) * blocks, 0)
                row[level, n] = pl.ds(pl.multiple_of(block * BLOCK, BLOCK), BLOCK)
        places.append(row)
    return places


def far_terms(places, far_refs, low_ref, high_ref, rows_ref, sums):
    count = range(len(places))
    kvs = [
        jnp.concatenate([far_refs[level][at, :] for (level, _), at in row.items()], axis=0)
        for row in places
    ]
    lows, highs = [low_ref[b] for b in count], [high_ref[b] for b in count]
    scores = [dot(kvs[b], lows[b], NT) for b in count]
    dweights = [dot(kvs[b], highs[b], NT) for b in count]
    weights = [jnp.exp(scores[b] - rows_ref[b, :1]) for b in count]
    dscores = [
        (weights[b] * (dweights[b] - rows_ref[b, 1:])).astype(jnp.bfloat16) for b in count
    ]
    weights = [one.astype(jnp.bfloat16) for one in weights]
    grad_qs = [dot(dscores[b], kvs[b], TN) for b in count]
    grad_kvs = [dot(dscores[b], lows[b]) + dot(weights[b], highs[b]) for b in count]
    for row, grad_kv in zip(places, grad_kvs):
        for n, ((level, _), at) in enumerate(row.items()):
            sums[level][at, :] += grad_kv[n * BLOCK : (n + 1) * BLOCK]
    return grad_qs


def comes_late(distances):
    return lax.axis_index(KV) - distances[1] >= lax.axis_size(KV) // 2


def far_kernel(distances, chosen_ref, low_ref, high_ref, rows_ref, part_ref, *refs):
    early_ref, traded_ref, fetched_ref, passed_ref, out_ref, *back_refs = refs[: 4 + LEVELS]
    four_ref, *totals = refs[4 + LEVELS :]
    sums = dict(zip(range(1, LEVELS), totals))
    at, quarter = lax.axis_index("z"), lax.axis_size("z") // 4
    in_second = jnp.logical_and(at >= quarter, at < 2 * quarter)
    four_ref[...] = jnp.where(in_second, traded_ref[...], fetched_ref[...])
    far_refs = {1: early_ref, 2: four_ref, 3: passed_ref}
    for total in totals:
        total[...] = jnp.zeros_like(total)
    blocks = low_ref.shape[0]
    is_late = comes_late(distances)

    def attend(levels):
        places = chosen_places(chosen_ref, distances, levels, blocks)
        grads = far_terms(places, far_refs, low_ref, high_ref, rows_ref, sums)
        for b, grad_q in enumerate(grads):
            out_ref[b] = part_ref[b] + grad_q

    pl.when(is_late)(lambda: attend((2, 3)))
    pl.when(jnp.logical_not(is_late))(lambda: attend((1, 2, 3)))
    for total, back_ref in zip(totals, back_refs):
        back_ref[...] = total[...].astype(back_ref.dtype)


def attend_far(distances, chosen, low, high, rows, part, far):
    kv = far[0]
    shape = (jax.ShapeDtypeStruct(part.shape, part.dtype),)
    shape += (jax.ShapeDtypeStruct(kv.shape, jnp.bfloat16),) * (LEVELS - 1)
    scratch = [pltpu.VMEM(kv.shape, kv.dtype)] + [pltpu.VMEM(kv.shape, jnp.float32)] * (LEVELS - 1)
    kernel = functools.partial(far_kernel, distances)
    args = (chosen, low, high, rows, part, *far)
    return call(kernel, 2 * 10**9, shape, *args, scratch=scratch)


def near_kernel(distances, chosen_ref, low_ref, high_ref, rows_ref, part_ref, *refs):
    one_ref, late_ref, found_ref, gq_ref, one_back_ref, two_back_ref, *totals = refs
    blocks, heads = low_ref.shape[0], low_ref.shape[1] // BLOCK
    lane = lax.broadcasted_iota(jnp.int32, (BLOCK, 2 * DH), 1)
    sums = dict(enumerate(totals))
    is_late = comes_late(distances)
    for total in totals:
        total[...] = jnp.zeros_like(total)

    def attend(levels):
        places = chosen_places(chosen_ref, distances, levels, blocks)
        near_refs = {0: one_ref, 1: late_ref}
        grads = far_terms(places, near_refs, low_ref, high_ref, rows_ref, sums)
        for b, grad_q in enumerate(grads):
            rows = slice(b * BLOCK, (b + 1) * BLOCK)
            grad_q = (part_ref[b] + grad_q) * DH ** (-0.5)
            for pair in range(heads // 2):
                first = grad_q[2 * pair * BLOCK : (2 * pair + 1) * BLOCK]
                second = grad_q[(2 * pair + 1) * BLOCK : (2 * pair + 2) * BLOCK]
                gq_ref[rows, pair * 2 * DH : (pair + 1) * 2 * DH] = jnp.where(
                    lane < DH, first, pltpu.roll(second, DH, 1)
                ).astype(gq_ref.dtype)

    pl.when(is_late)(lambda: attend((0, 1)))
    pl.when(jnp.logical_not(is_late))(lambda: attend((0,)))
    one_back_ref[...] = totals[0][...].astype(one_back_ref.dtype)
    two_back = totals[1][...].astype(two_back_ref.dtype)
    two_back_ref[...] = jnp.where(is_late, two_back, found_ref[...])


def attend_near(distances, chosen, low, high, rows, part, near, late, found):
    tokens, width = low.shape[0] * BLOCK, low.shape[1] * DH // BLOCK
    shape = (jax.ShapeDtypeStruct((tokens, width), jnp.bfloat16),)
    shape += (jax.ShapeDtypeStruct(near.shape, jnp.bfloat16),) * 2
    kernel = functools.partial(near_kernel, distances)
    args = (chosen, low, high, rows, part, near, late, found)
    scratch = [pltpu.VMEM(near.shape, jnp.float32)] * 2
    return call(kernel, 10**9, shape, *args, scratch=scratch)


def weight_kernel(mine_ref, other_ref, x_ref, out_ref, held, done):
    core = lax.axis_index("c")
    peers = x_ref.shape[0] // 2
    ys = out_ref.shape[0]
    step = x_ref.shape[2] // ys
    grads = jnp.concatenate([mine_ref[...], other_ref[...]], axis=0)
    copies = []
    for half in range(2):
        mine = range(half * ys // 2, (half + 1) * ys // 2)
        lanes = slice(mine[0] * step, (mine[-1] + 1) * step)
        for peer in range(peers):
            slots = [X_ORDER.index(c * peers + peer) for c in range(2)]
            first, second = jnp.where(core == 0, *slots), jnp.where(core == 0, *slots[::-1])
            x = jnp.concatenate([x_ref[first, :, lanes], x_ref[second, :, lanes]], axis=0)
            part = dot(x, grads, TN).astype(held.dtype)
            for n, y in enumerate(mine):
                held[y, peer * step : (peer + 1) * step] = part[n * step : (n + 1) * step]
        for y in mine:
            slot = jnp.where(core == 0, *(order.index(y) for order in Y_ORDERS))
            copies.append(pltpu.make_async_copy(held.at[y], out_ref.at[slot], done.at[y]))
            copies[-1].start()
    for copy in copies:
        copy.wait()


def weight(mine, other, x, ys):
    peers, tokens, part = x.shape[0] // 2, x.shape[1], x.shape[2]
    shape = (ys, peers * part // ys, mine.shape[1])
    vmem = pl.BlockSpec(memory_space=pltpu.VMEM)
    return pl.pallas_call(
        weight_kernel,
        out_shape=jax.ShapeDtypeStruct(shape, jnp.bfloat16),
        in_specs=[vmem] * 3,
        out_specs=pl.BlockSpec(memory_space=pltpu.HBM),
        scratch_shapes=[pltpu.VMEM(shape, jnp.bfloat16), pltpu.SemaphoreType.DMA((ys,))],
        cost_estimate=pl.CostEstimate(
            flops=4 * tokens * peers * part * mine.shape[1], bytes_accessed=10**6, transcendentals=0
        ),
        compiler_params=pltpu.CompilerParams(vmem_limit_bytes=VMEM_LIMIT),
        name="weight",
    )(mine, other, x)


def sum_kernel(order, tiles_ref, out_ref):
    total = tiles_ref[0].astype(jnp.float32)
    for n in range(1, tiles_ref.shape[0]):
        total = total + tiles_ref[n].astype(jnp.float32)
    total = total.astype(out_ref.dtype)
    if order is None:
        out_ref[...] = total
    else:
        for slot, place in enumerate(order):
            out_ref[slot] = total[place]


def summed(tiles, dtype, order=None):
    shape = jax.ShapeDtypeStruct(tiles.shape[1:], dtype)
    return call(functools.partial(sum_kernel, order), tiles.size, shape, tiles)


def collect_kernel(grads_ref, own_ref, *refs):
    *parts, gq_ref, gk_ref, gv_ref = refs
    total = own_ref[...]
    for ref in parts:
        total = total + ref[...].astype(jnp.float32)
    total = turned(total)
    width = total.shape[0] // 2
    gq_ref[...] = grads_ref[...]
    gk_ref[...] = total[:width].astype(jnp.bfloat16)
    gv_ref[...] = total[width:].astype(jnp.bfloat16)


def collect(grads, own, back):
    shape = jax.ShapeDtypeStruct((own.shape[1] // 2, own.shape[0]), jnp.bfloat16)
    shapes = (jax.ShapeDtypeStruct(grads.shape, grads.dtype), shape, shape)
    return call(collect_kernel, 10**6, shapes, grads, own, *back)


def shards(layer_input, queries, keys, values, attn_out, grad_out, log_sum, chosen):
    axis_size = lax.axis_size(KV)
    ys, cores, peers = lax.axis_size("y"), lax.axis_size("c"), lax.axis_size("x")
    out_rows = layer_input.shape[1] * peers // axis_size
    distances = [1, axis_size // 8, axis_size // 4, axis_size // 2]
    key_pair = pack(keys.T, values.T)
    near = shifted(key_pair, KV, distances[0])
    halves = [range(axis_size // 2), range(axis_size // 2, axis_size)]
    steps = []
    for senders in halves:
        steps.append(shifted(key_pair, KV, distances[1], senders))
    quarter = lax.axis_size("z") // 4
    quarters = [range(n * quarter, (n + 1) * quarter) for n in range(4)]
    traded = between(key_pair, quarters, ((0, 1), (1, 0)))
    passed = between(traded, quarters, ((1, 2), (0, 3)))
    fetched = between(key_pair, quarters, ((1, 2), (2, 3)))
    far = [steps[0], traded, fetched, passed]
    sent = spread(layer_input, out_rows, ys, cores, peers)
    whole_input = exchanged(sent, ("c", "x"), [list(X_ORDER)])
    *staged, part, grad_own = attend_own(queries, grad_out, attn_out, log_sum.T, key_pair)
    part, found, *back_far = attend_far(distances, chosen.T, *staged, part, far)
    near = (near, steps[1], found)
    grads, *back = attend_near(distances, chosen.T, *staged, part, *near)
    back += back_far
    route = [(i, cores - 1 - i) for i in range(cores)]
    other = lax.ppermute(grads, "c", route)
    parts = weight(grads, other, whole_input, ys)
    groups = [[y * cores + c for y in order] for c, order in enumerate(Y_ORDERS)]
    over_y = exchanged(parts, ("y", "c"), groups)
    returned = []
    for level, distance in enumerate(distances[:-1]):
        for receivers in halves:
            block = shifted(back[level], KV, -distance, receivers=receivers)
            returned.append(block)
    returned.append(shifted(back[-1], KV, -distances[-1]))
    over_y = summed(over_y.reshape(ys, -1, out_rows, over_y.shape[2]), jnp.bfloat16, Z_ORDER)
    over_z = exchanged(over_y, "z", [list(Z_ORDER)])
    grad_queries, grad_keys, grad_values = collect(grads, grad_own, returned)
    grad_weight = summed(over_z, jnp.float32)
    return (grad_queries, grad_keys.T, grad_values.T, grad_weight)


def solution(mesh):
    ys, cores = SIDES
    shape = (mesh.shape["kv"] // (ys * cores), ys, cores, mesh.shape["tp"])
    torus = Mesh(mesh.devices.reshape(shape), (*KV, "x"))
    return jax.shard_map(
        shards,
        mesh=torus,
        in_specs=(P(KV, "x"),) * 7 + (P(),),
        out_specs=(P(KV, "x"),) * 4,
        check_vma=False,
    )
```
